256 devices in a mesh: sp: 32 (over z, y), tp: 8 (over x, core).
Axes of the slice: x: 4, y: 4, z: 8, core: 2. Of those that a mesh axis runs over, the one named last changes fastest.
Arguments:
- activations: bfloat16 [24576, 2048], P(('sp', 'tp')), may hold values from -6 to 6
- in_gain: float32 [2048], replicated, may hold values from 0.1 to 1.9
- w_pool_in: bfloat16 [2048, 1024], P(None, 'tp'), may hold values from -0.125 to 0.125
- pool_gain: float32 [1024], P('tp'), may hold values from 0.1 to 1.9
- w_qlat: bfloat16 [2048, 768], P(None, 'tp'), may hold values from -0.125 to 0.125
- w_kvlat: bfloat16 [2048, 512], P(None, 'tp'), may hold values from -0.125 to 0.125
- w_krope: bfloat16 [2048, 32], replicated, may hold values from -0.125 to 0.125
- qlat_gain: float32 [768], replicated, may hold values from 0.1 to 1.9
- kvlat_gain: float32 [512], replicated, may hold values from 0.1 to 1.9
- w_qup: bfloat16 [768, 1536], P(None, 'tp'), may hold values from -0.21875 to 0.21875
- w_kup: bfloat16 [512, 1024], P(None, 'tp'), may hold values from -0.25 to 0.25
- w_vup: bfloat16 [512, 1024], P(None, 'tp'), may hold values from -0.25 to 0.25
- qhead_gain: float32 [96], replicated, may hold values from 1.1 to 1.9
- khead_gain: float32 [96], replicated, may hold values from 1.1 to 1.9
- w_out_pool: bfloat16 [1024, 2048], P('tp'), may hold values from -0.1875 to 0.1875
- w_out_attn: bfloat16 [1024, 2048], P('tp'), may hold values from -0.75 to 0.75
Outputs:
- mixed: bfloat16 [24576, 2048], P(('sp', 'tp'))
The draws below stay inside these ranges and needn't reach their ends.
All inputs are finite; a program needn't handle non-finite values.
Results may differ from the reference program's by a relative error of at most 0.025.
Values may be sent and summed in bfloat16 or wider, within the bound.
A program may use at most 128 MiB of HBM per device.

```python
import math
import jax
import jax.numpy as jnp
from jax import lax

D = 2048
POOL = 1024
GROUP = 256
HEADS = 16
NOPE = 64
ROPE = 32
VDIM = 64
QLAT = 768
KVLAT = 512
TOKENS = 24576
N_TP = 8


def level_of(stream_key, extent, split, low, top_value):
    def one(axis_at, shards_of):
        draws = jax.random.uniform(jax.random.fold_in(jax.random.fold_in(stream_key, 6), axis_at), (shards_of,), jnp.float32, low / len(split), top_value / len(split))
        return jnp.repeat(jnp.exp(draws), extent[axis_at] // shards_of).reshape((-1,) + (1,) * (len(extent) - axis_at - 1))

    level = one(*split[0])
    for cut in split[1:]:
        level = level * one(*cut)
    return level


def noise(own_key, shape, scale, reach, cuts=(), kind=jnp.bfloat16):
    array = jax.random.normal(own_key, shape, jnp.float32) * scale
    if len(cuts) > 0:
        array = level_of(own_key, shape, cuts, -0.22, 0.18) * array
    return jnp.clip(array, min=-reach, max=reach).astype(kind)


def setup_inputs(seed: int = 0) -> dict:
    streams_of = jax.random.split(jax.random.key(seed), 17)
    activations = noise(streams_of[0], (TOKENS, D), 1.0, 6.0, ((0, 256),))
    in_gain = jnp.clip(1.0 + 0.18 * jax.random.normal(streams_of[1], (D,), jnp.float32), 0.1, 1.9)
    w_pool_in = noise(streams_of[2], (D, POOL), D ** -0.5, 0.125, ((1, 8),))
    pool_gain = jnp.clip(1.0 + 0.18 * jax.random.normal(streams_of[3], (POOL,), jnp.float32), 0.1, 1.9)
    w_qlat = noise(streams_of[4], (D, QLAT), D ** -0.5, 0.125, ((1, 8),))
    w_kvlat = noise(streams_of[5], (D, KVLAT), D ** -0.5, 0.125, ((1, 8),))
    w_krope = noise(streams_of[6], (D, ROPE), D ** -0.5, 0.125)
    qlat_gain = jnp.clip(1.0 + 0.18 * jax.random.normal(streams_of[7], (QLAT,), jnp.float32), 0.1, 1.9)
    kvlat_gain = jnp.clip(1.0 + 0.18 * jax.random.normal(streams_of[8], (KVLAT,), jnp.float32), 0.1, 1.9)
    w_qup = noise(streams_of[9], (QLAT, HEADS * (NOPE + ROPE)), QLAT ** -0.5, 0.21875, ((1, 8),))
    w_kup = noise(streams_of[10], (KVLAT, HEADS * NOPE), KVLAT ** -0.5, 0.25, ((1, 8),))
    w_vup = noise(streams_of[11], (KVLAT, HEADS * VDIM), KVLAT ** -0.5, 0.25, ((1, 8),))
    qhead_gain = jnp.clip(jax.random.uniform(streams_of[12], (NOPE + ROPE,), jnp.float32, 1.1, 1.9), 1.1, 1.9)
    khead_gain = jnp.clip(jax.random.uniform(streams_of[13], (NOPE + ROPE,), jnp.float32, 1.1, 1.9), 1.1, 1.9)
    w_out_pool = noise(streams_of[14], (POOL, D), POOL ** -0.5, 0.1875, ((0, 8),))
    w_out_attn = noise(streams_of[15], (HEADS * VDIM, D), (HEADS * VDIM // 16) ** -0.5, 0.75, ((0, 8),))
    return {"activations": activations, "in_gain": in_gain, "w_pool_in": w_pool_in, "pool_gain": pool_gain, "w_qlat": w_qlat, "w_kvlat": w_kvlat, "w_krope": w_krope, "qlat_gain": qlat_gain, "kvlat_gain": kvlat_gain, "w_qup": w_qup, "w_kup": w_kup, "w_vup": w_vup, "qhead_gain": qhead_gain, "khead_gain": khead_gain, "w_out_pool": w_out_pool, "w_out_attn": w_out_attn}


norm_eps = 1e-06
rope_theta = 10000.0
rim_depth = 15
block_rows = 512

def row_norm(source, norm_gain):
    as_float = source.astype(jnp.float32)
    factor = lax.rsqrt(lax.optimization_barrier(jnp.mean(as_float * as_float, axis=-1, keepdims=True)) + norm_eps)
    return as_float * factor * norm_gain

def rotate(head_rows, positions):
    half_rope = ROPE // 2
    frequency = rope_theta ** (-jnp.arange(0, ROPE, 2, dtype=jnp.float32) / ROPE)
    angles = positions.astype(jnp.float32)[:, None] * frequency[None, :]
    cosine = jnp.cos(angles)[:, None, :]
    sine_part = jnp.sin(angles)[:, None, :]
    plain_part = head_rows[..., :NOPE]
    lower_half = head_rows[..., NOPE:NOPE + half_rope]
    upper_half = head_rows[..., NOPE + half_rope:]
    return jnp.concatenate([plain_part, lower_half * cosine - upper_half * sine_part, upper_half * cosine + lower_half * sine_part], axis=-1)

def pool_mix(extended, positions, channel_start):
    row_count = positions.shape[0]
    width = extended.shape[1]
    channel = channel_start + jnp.arange(width, dtype=jnp.int32)
    window = jnp.left_shift(jnp.int32(2), (channel // GROUP).astype(jnp.int32))
    as_float = extended.astype(jnp.float32)
    window_sum = jnp.zeros((row_count, width), jnp.float32)
    for lag_index in range(rim_depth + 1):
        lagged = as_float[rim_depth - lag_index:rim_depth - lag_index + row_count]
        window_sum = window_sum + jnp.where(lag_index < window[None, :], lagged, 0.0)
    divisor = jnp.minimum(positions[:, None] + 1, window[None, :]).astype(jnp.float32)
    return window_sum / divisor - as_float[rim_depth:]

def make_queries(q_normed, w_qup, norm_gain, positions):
    row_count = q_normed.shape[0]
    head_count = w_qup.shape[1] // (NOPE + ROPE)
    query_raw = jnp.dot(q_normed, w_qup, preferred_element_type=jnp.float32).astype(jnp.bfloat16)
    query_raw = query_raw.reshape(row_count, head_count, NOPE + ROPE)
    return rotate(row_norm(query_raw, norm_gain), positions).astype(jnp.bfloat16)

def make_keys(kv_rows, rope_rows, w_kup, w_vup, norm_gain, positions):
    row_count = kv_rows.shape[0]
    head_count = w_kup.shape[1] // NOPE
    key_plain = jnp.dot(kv_rows, w_kup, preferred_element_type=jnp.float32).astype(jnp.bfloat16)
    key_plain = key_plain.reshape(row_count, head_count, NOPE)
    value_rows = jnp.dot(kv_rows, w_vup, preferred_element_type=jnp.float32).astype(jnp.bfloat16)
    shared = jnp.broadcast_to(rope_rows[:, None, :], (row_count, head_count, ROPE))
    joined = jnp.concatenate([key_plain, shared], axis=-1)
    key_rows = rotate(row_norm(joined, norm_gain), positions).astype(jnp.bfloat16)
    return (key_rows.reshape(row_count, head_count * (NOPE + ROPE)), value_rows)

def attend(queries, key_rows, value_rows):
    all_rows, head_count, _ = queries.shape
    block_size = math.gcd(block_rows, all_rows)
    key_rows = key_rows.reshape(all_rows, head_count, NOPE + ROPE)
    value_rows = value_rows.reshape(all_rows, head_count, VDIM)
    score_scale = (NOPE + ROPE) ** (-0.5)

    def one_block(block_index):
        first_row = block_index * block_size
        query_block = lax.dynamic_slice_in_dim(queries, first_row, block_size, 0).astype(jnp.float32)
        query_pos = first_row + jnp.arange(block_size, dtype=jnp.int32)

        def add_keys(key_index, state_pair):
            numerator, denominator = state_pair
            key_first = key_index * block_size
            key_block = lax.dynamic_slice_in_dim(key_rows, key_first, block_size, 0).astype(jnp.float32)
            value_block = lax.dynamic_slice_in_dim(value_rows, key_first, block_size, 0).astype(jnp.float32)
            key_pos = key_first + jnp.arange(block_size, dtype=jnp.int32)
            scores = jnp.einsum('qhd,khd->hqk', query_block, key_block) * score_scale
            weights = jnp.where(key_pos[None, None, :] <= query_pos[None, :, None], jnp.exp(scores), 0.0)
            denominator = denominator + lax.optimization_barrier(jnp.sum(weights, axis=-1))
            rounded = lax.optimization_barrier(weights.astype(jnp.bfloat16)).astype(jnp.float32)
            numerator = numerator + jnp.einsum('hqk,khd->qhd', rounded, value_block)
            return (numerator, denominator)
        start_pair = (jnp.zeros((block_size, head_count, VDIM), jnp.float32), jnp.zeros((head_count, block_size), jnp.float32))
        numerator, denominator = lax.fori_loop(0, block_index + 1, add_keys, start_pair)
        return (numerator / jnp.transpose(denominator)[:, :, None]).astype(jnp.bfloat16)
    blocks_out = lax.map(one_block, jnp.arange(all_rows // block_size, dtype=jnp.int32))
    return blocks_out.reshape(all_rows, head_count * VDIM)

def reference(activations, in_gain, w_pool_in, pool_gain, w_qlat, w_kvlat, w_krope, qlat_gain, kvlat_gain, w_qup, w_kup, w_vup, qhead_gain, khead_gain, w_out_pool, w_out_attn):
    positions = jnp.arange(TOKENS, dtype=jnp.int32)
    normed = row_norm(activations, in_gain).astype(jnp.bfloat16)
    pool_in = jnp.dot(normed, w_pool_in, preferred_element_type=jnp.float32).astype(jnp.bfloat16)
    extended = jnp.concatenate([jnp.zeros((rim_depth, POOL), jnp.bfloat16), pool_in], axis=0)
    pool_out = (pool_mix(extended, positions, 0) * pool_gain).astype(jnp.bfloat16)
    q_latent = jnp.dot(normed, w_qlat, preferred_element_type=jnp.float32).astype(jnp.bfloat16)
    kv_latent = jnp.dot(normed, w_kvlat, preferred_element_type=jnp.float32).astype(jnp.bfloat16)
    rope_key = jnp.dot(normed, w_krope, preferred_element_type=jnp.float32).astype(jnp.bfloat16)
    q_normed = row_norm(q_latent, qlat_gain).astype(jnp.bfloat16)
    kv_normed = row_norm(kv_latent, kvlat_gain).astype(jnp.bfloat16)
    queries = make_queries(q_normed, w_qup, qhead_gain, positions)
    key_rows, value_rows = make_keys(kv_normed, rope_key, w_kup, w_vup, khead_gain, positions)
    attended = attend(queries, key_rows, value_rows)
    pool_span = POOL // N_TP
    attn_span = HEADS * VDIM // N_TP
    mixed = jnp.zeros((TOKENS, D), jnp.float32)
    for block_index in range(N_TP):
        pool_lo = block_index * pool_span
        attn_lo = block_index * attn_span
        partial_value = jnp.dot(pool_out[:, pool_lo:pool_lo + pool_span], w_out_pool[pool_lo:pool_lo + pool_span], preferred_element_type=jnp.float32)
        partial_value = partial_value + jnp.dot(attended[:, attn_lo:attn_lo + attn_span], w_out_attn[attn_lo:attn_lo + attn_span], preferred_element_type=jnp.float32)
        rounded = lax.optimization_barrier(partial_value.astype(jnp.bfloat16)).astype(jnp.float32)
        mixed = mixed + rounded
    return mixed.astype(jnp.bfloat16)
```

```python
import functools
import math

import jax
import jax.numpy as jnp
import numpy as np
from jax import lax
from jax.experimental import pallas as pl
from jax.experimental.pallas import tpu as pltpu
from jax.sharding import PartitionSpec as P

NOPE = 64
ROPE = 32
HEAD = NOPE + ROPE
VDIM = 64
QLAT = 768
KVLAT = 512
EPS = 1e-06
THETA = 10000.0
ROWS = 768
BLOCK = 96
HALF = BLOCK // 2
D = 2048
LAT = 160
HALO = 16
F32 = jnp.float32
BF16 = jnp.bfloat16
MESH = pl.DeviceIdType.MESH
VMEM_SPEC = pl.BlockSpec(memory_space=pltpu.VMEM)
SCALE = (1.0 / math.sqrt(HEAD)) * math.log2(math.e)


def dot(a, b):
    return jnp.dot(a, b, preferred_element_type=F32)


def turned(a):
    return jnp.transpose(a.astype(F32))


def rotary_tables():
    freq = THETA ** (-np.arange(0, ROPE, 2, dtype=np.float64) / ROPE)
    far = freq[:, None] * (np.arange(128, dtype=np.float64)[None, :] * ROWS)
    near = freq[:, None] * np.arange(ROWS, dtype=np.float64)[None, :]
    return tuple(t.astype(np.float32) for t in (np.cos(far), np.sin(far), np.cos(near), np.sin(near)))


def place():
    sp = lax.axis_index("sp")
    tp = lax.axis_index("tp")
    return sp, tp, tp // 2, lax.rem(tp, 2)


def meet(devices):
    barrier = pltpu.get_barrier_semaphore()
    for device in devices:
        pl.semaphore_signal(barrier, inc=1, device_id=device, device_id_type=MESH)
    pl.semaphore_wait(barrier, len(devices))


def remote(src, dst, send_sem, recv_sem, device):
    return pltpu.make_async_remote_copy(
        src_ref=src, dst_ref=dst, send_sem=send_sem, recv_sem=recv_sem, device_id=device, device_id_type=MESH
    )


class TpGather:
    def __init__(self, own, everything, half, sp, x, c, ring_send, sib_send, recv):
        self.own, self.all, self.half = own, everything, half
        self.x, self.c = x, c
        self.ring_send, self.sib_send, self.recv = ring_send, sib_send, recv
        self.right = {"sp": sp, "tp": lax.rem(x + 1, 4) * 2 + c}
        self.left = {"sp": sp, "tp": lax.rem(x + 3, 4) * 2 + c}
        self.sib = {"sp": sp, "tp": x * 2 + 1 - c}

    def index(self, offset, core):
        return lax.rem(self.x + 4 + offset, 4) * 2 + core

    def rows(self, h):
        return pl.ds(h * self.half, self.half)

    def piece(self, idx, h):
        return self.all.at[idx, self.rows(h)]

    def copy(self, src, idx, h, send, device):
        return remote(src, self.piece(idx, h), send, self.recv.at[idx, h], device)

    def start(self):
        me = self.index(0, self.c)
        for k, (device, h) in enumerate(((self.right, 0), (self.left, 1), (self.right, 1), (self.left, 0))):
            self.copy(self.own.at[self.rows(h)], me, h, self.ring_send.at[k], device).start()
        for h in range(2):
            self.copy(self.own.at[self.rows(h)], me, h, self.sib_send.at[h], self.sib).start()

    def wait_piece(self, idx, h):
        self.copy(self.own.at[self.rows(h)], idx, h, self.sib_send.at[0], self.sib).wait_recv()

    def got(self, offset, h, slot, onward=None, onward_slot=0):
        idx = self.index(offset, self.c)
        self.wait_piece(idx, h)
        if onward is not None:
            self.copy(self.piece(idx, h), idx, h, self.ring_send.at[onward_slot], onward).start()
        self.copy(self.piece(idx, h), idx, h, self.sib_send.at[slot], self.sib).start()

    def relay_near(self):
        self.got(-1, 0, 2, self.right, 4)
        self.got(1, 1, 3, self.left, 5)
        self.got(-1, 1, 4)
        self.got(1, 0, 5)

    def relay_far(self):
        self.got(2, 0, 6)
        self.got(2, 1, 7)

    def wait_sibling(self, offset):
        idx = self.index(offset, 1 - self.c)
        for h in range(2):
            self.wait_piece(idx, h)
        return idx

    def finish(self):
        for k in range(6):
            self.copy(self.own.at[self.rows(0)], 0, 0, self.ring_send.at[k], self.sib).wait_send()
        for k in range(8):
            self.copy(self.own.at[self.rows(0)], 0, 0, self.sib_send.at[k], self.sib).wait_send()


def front_kernel(
    act, in_gain, w_pool, w_lat, pool_gain, q_gain, kv_gain, w_qup, w_kup, w_vup, qh_gain, kh_gain,
    far_cos, far_sin, near_cos, near_sin,
    q_out, kv_out, pool_out,
    act_all, lat_rows, lat_own, lat_all, pool_rows, halo_out, halo_in, wq_t, wkv_t,
    a_ring, a_sib, a_recv, l_ring, l_sib, l_recv, halo_sem,
):
    sp, tp, x, c = place()
    acts = TpGather(act, act_all, HALF, sp, x, c, a_ring, a_sib, a_recv)
    lats = TpGather(lat_own, lat_all, LAT // 2, sp, x, c, l_ring, l_sib, l_recv)
    behind = {"sp": lax.rem(sp + 1, 32), "tp": tp}
    before = {"sp": lax.rem(sp + 31, 32), "tp": tp}
    meet([acts.right, acts.left, acts.sib, behind, before])
    acts.start()

    def project(block, idx):
        rows = pl.multiple_of(idx * BLOCK, 32)
        value = block[...].astype(F32)
        factor = lax.rsqrt(jnp.mean(value * value, axis=1, keepdims=True) + EPS)
        normed = (value * factor * in_gain[...]).astype(BF16)
        pool_rows[pl.ds(HALO + rows, BLOCK), :] = dot(normed, w_pool[...]).astype(BF16).astype(F32)
        lat_rows[pl.ds(rows, BLOCK), :] = dot(normed, w_lat[...])

    project(act, tp)
    wq_t[...] = turned(w_qup[...]).astype(BF16)
    wkv_t[pl.ds(0, 128), :] = turned(w_kup[...]).astype(BF16)
    wkv_t[pl.ds(128, 128), :] = turned(w_vup[...]).astype(BF16)
    idx = acts.wait_sibling(0)
    project(act_all.at[idx], idx)
    acts.relay_near()
    for offset in (-1, 1):
        idx = acts.index(offset, c)
        project(act_all.at[idx], idx)
    for offset in (-1, 1):
        idx = acts.wait_sibling(offset)
        project(act_all.at[idx], idx)
    acts.relay_far()
    idx = acts.index(2, c)
    project(act_all.at[idx], idx)
    idx = acts.wait_sibling(2)
    project(act_all.at[idx], idx)

    lat_t = jnp.transpose(lat_rows[...])
    lat_own[...] = lat_t[:LAT].astype(BF16)
    rope_t = lat_t[LAT:].astype(BF16).astype(F32)
    halo_out[...] = pool_rows[pl.ds(ROWS, HALO), :].astype(BF16)
    lats.start()
    halo = remote(halo_out, halo_in, halo_sem.at[0], halo_sem.at[1], behind)
    halo.start()
    lat_all[tp] = lat_own[...]

    cos = jnp.sum(jnp.where(lax.broadcasted_iota(jnp.int32, (16, 128), 1) == sp, far_cos[...], 0.0), axis=1, keepdims=True)
    sin = jnp.sum(jnp.where(lax.broadcasted_iota(jnp.int32, (16, 128), 1) == sp, far_sin[...], 0.0), axis=1, keepdims=True)
    cosine = cos * near_cos[...] - sin * near_sin[...]
    sine = sin * near_cos[...] + cos * near_sin[...]

    halo.wait_recv()
    pool_rows[pl.ds(0, HALO), :] = jnp.where(sp > 0, halo_in[...].astype(F32), 0.0)
    window = jnp.left_shift(jnp.int32(2), tp // 2)
    total = jnp.zeros((ROWS, 128), F32)
    for lag in range(16):
        total = total + jnp.where(lag < window, pool_rows[pl.ds(HALO - lag, ROWS), :], 0.0)
    position = sp * ROWS + lax.broadcasted_iota(jnp.int32, (ROWS, 128), 0)
    divisor = jnp.minimum(position + 1, window).astype(F32)
    pooled = total / divisor - pool_rows[pl.ds(HALO, ROWS), :]
    pool_out[...] = (pooled * pool_gain[...]).astype(BF16)

    lats.relay_near()
    lats.relay_far()
    for offset in (0, -1, 1, 2):
        lats.wait_sibling(offset)

    q_lat = lat_all[:, 0:96, :].reshape(QLAT, ROWS).astype(F32)
    q_norm = q_lat * lax.rsqrt(jnp.sum(q_lat * q_lat, axis=0, keepdims=True) / QLAT + EPS) * q_gain[...]
    raw = dot(wq_t[...], q_norm.astype(BF16)).astype(BF16).astype(F32)
    kv_lat = lat_all[:, 96:LAT, :].reshape(KVLAT, ROWS).astype(F32)
    kv_norm = kv_lat * lax.rsqrt(jnp.sum(kv_lat * kv_lat, axis=0, keepdims=True) / KVLAT + EPS) * kv_gain[...]
    plain = dot(wkv_t[...], kv_norm.astype(BF16)).astype(BF16)

    def finish(head, gain):
        factor = lax.rsqrt(jnp.sum(head * head, axis=0, keepdims=True) / HEAD + EPS)
        head = head * factor * gain
        lower, upper = head[64:80], head[80:96]
        return jnp.concatenate([head[:64], lower * cosine - upper * sine, upper * cosine + lower * sine], axis=0)

    for h in range(2):
        q_out[h] = (finish(raw[h * 96 : h * 96 + 96], qh_gain[...]) * SCALE).astype(BF16)
        joined = jnp.concatenate([plain[h * 64 : h * 64 + 64].astype(F32), rope_t], axis=0)
        kv_out[h, 0:96, :] = finish(joined, kh_gain[...]).astype(BF16)
        kv_out[h, 96:160, :] = plain[128 + h * 64 : 192 + h * 64]
    acts.finish()
    lats.finish()
    halo.wait_send()


def attend_kernel(
    q_ref, kv_ref, att_ref,
    kv_all, k_rows, q_in, acc, den, o_stage, att_in,
    c_send, kv_recv, q_send, q_recv, ring_send, sib_send, o_send, o_recv,
):
    sp, tp, x, c = place()
    z, y = sp // 4, lax.rem(sp, 4)

    def device(yy, zz, cc):
        return {"sp": zz * 4 + yy, "tp": x * 2 + cc}

    up = device(y, lax.rem(z + 1, 8), c)
    down = device(y, lax.rem(z + 7, 8), c)
    sib = device(y, z, 1 - c)
    friends = [up, down]
    for dy in range(4):
        for dc in range(2):
            yy, cc = lax.rem(y + dy, 4), lax.rem(c + dc, 2)
            friends.append(device(yy, 7 - z, cc))
            if dy or dc:
                friends.append(device(yy, z, cc))
    meet(friends)

    even = lax.rem(y, 2) == 0
    owner = y // 2
    part = lax.rem(y, 2)

    def kv_copy(j):
        return remote(kv_ref.at[j], kv_all.at[sp], c_send.at[j], kv_recv.at[sp], device(2 * c + j, z, owner))

    def q_copy(j):
        to_z = jnp.where(even, z, 7 - z)
        to_c = jnp.where(even, owner, (3 - y) // 2)
        return remote(q_ref.at[j], q_in.at[part], q_send.at[j], q_recv.at[part], device(2 * c + j, to_z, to_c))

    for j in range(2):
        here = 2 * c + j == y

        @pl.when(jnp.logical_not(here))
        def _():
            kv_copy(j).start()

        @pl.when(here)
        def _():
            kv_all[sp] = kv_ref[j]

    for j in range(2):
        here = jnp.logical_and(even, 2 * c + j == y)

        @pl.when(jnp.logical_not(here))
        def _():
            q_copy(j).start()

        @pl.when(here)
        def _():
            q_in[0] = q_ref[j]

    acc[...] = jnp.zeros_like(acc)
    den[...] = jnp.zeros_like(den)

    def wait_slot(slot):
        remote(kv_all.at[slot], kv_all.at[slot], sib_send.at[slot], kv_recv.at[slot], sib).wait_recv()

    def ring_copy(slot, way, b, s):
        return remote(kv_all.at[slot], kv_all.at[slot], ring_send.at[way, b, s], kv_recv.at[slot], (up, down)[way])

    def sib_copy(slot):
        return remote(kv_all.at[slot], kv_all.at[slot], sib_send.at[slot], kv_recv.at[slot], sib)

    def attend(slot, qb, diagonal):
        for qc in range(3):
            columns = pl.ds(qc * 256, 256)
            keys = (qc + 1) * 256 if diagonal else ROWS
            scores = dot(k_rows[slot, pl.ds(0, keys), :], q_in[qb, :, columns])
            weights = jnp.exp2(scores)
            if diagonal:
                k_pos = lax.broadcasted_iota(jnp.int32, (keys, 256), 0)
                q_pos = lax.broadcasted_iota(jnp.int32, (keys, 256), 1) + qc * 256
                weights = jnp.where(k_pos <= q_pos, weights, 0.0)
            den[qb, :, columns] += jnp.sum(weights.reshape(keys // 8, 8, 256), axis=0)
            acc[qb, :, columns] += dot(kv_all[slot, pl.ds(96, 64), pl.ds(0, keys)], weights.astype(BF16))

    q_index = (z * 4 + 2 * c, (7 - z) * 4 + 3 - 2 * c)

    def plane_of(way, s):
        return lax.rem(z + 8 - s, 8) if way == 0 else lax.rem(z + s, 8)

    @pl.loop(0, 5)
    def _(s):
        for b in range(2):
            @pl.when(jnp.logical_and(s == 0, 2 * c + b != y))
            def _():
                wait_slot(z * 4 + 2 * c + b)

        for b in range(2):
            for way in ((0, 1), (1, 0))[b]:
                limit = 4 if way == b else 3
                slot = plane_of(way, s) * 4 + 2 * c + b

                @pl.when(jnp.logical_and(s >= 1, s <= limit))
                def _():
                    wait_slot(slot)

                @pl.when(s < limit)
                def _():
                    ring_copy(slot, way, b, s).start()

                @pl.when(jnp.logical_and(jnp.logical_or(s >= 1, way == 0), s <= limit))
                def _():
                    sib_copy(slot).start()

        @pl.when(jnp.logical_and(s == 0, 2 * c != y))
        def _():
            remote(q_ref.at[0], q_in.at[0], q_send.at[0], q_recv.at[0], sib).wait_recv()

        @pl.when(s == 0)
        def _():
            remote(q_ref.at[0], q_in.at[1], q_send.at[0], q_recv.at[1], sib).wait_recv()

        planes = jnp.where(jnp.logical_and(s >= 1, s <= 3), 2, 1)

        @pl.loop(0, planes)
        def _(side):
            zb = lax.rem(z + 8 + jnp.where(side == 0, -s, s), 8)
            for b in range(2):
                wait_slot(zb * 4 + 2 * (1 - c) + b)

            @pl.loop(0, 4)
            def _(yb):
                slot = zb * 4 + yb
                needed = slot <= jnp.maximum(q_index[0], q_index[1])

                @pl.when(needed)
                def _():
                    k_rows[slot] = turned(kv_all[slot, pl.ds(0, HEAD), :]).astype(BF16)

                @pl.loop(0, 2)
                def _(qb):
                    query = jnp.where(qb == 0, q_index[0], q_index[1])

                    @pl.when(slot < query)
                    def _():
                        attend(slot, qb, False)

                    @pl.when(slot == query)
                    def _():
                        attend(slot, qb, True)

    def back(qb):
        to_y, to_z = (2 * c, z) if qb == 0 else (3 - 2 * c, 7 - z)
        return remote(o_stage.at[qb], att_in.at[part], o_send.at[qb], o_recv.at[part], device(to_y, to_z, owner))

    for qb in range(2):
        o_stage[qb] = (acc[qb] / jnp.sum(den[qb], axis=0, keepdims=True)).astype(BF16)

    @pl.when(2 * c == y)
    def _():
        att_in[part] = o_stage[0]

    @pl.when(2 * c != y)
    def _():
        back(0).start()

    back(1).start()

    for j in range(2):
        @pl.when(jnp.logical_not(jnp.logical_and(even, 2 * c + j == y)))
        def _():
            remote(o_stage.at[0], att_in.at[j], o_send.at[0], o_recv.at[j], sib).wait_recv()
            q_copy(j).wait_send()

        @pl.when(2 * c + j != y)
        def _():
            kv_copy(j).wait_send()

    att_ref[...] = att_in[...]

    @pl.when(2 * c != y)
    def _():
        back(0).wait_send()

    back(1).wait_send()
    for b in range(2):
        for way in range(2):
            for s in range(4 if way == b else 3):
                ring_copy(0, way, b, s).wait_send()

    @pl.loop(0, 8)
    def _(zb):
        for b in range(2):
            sib_copy(zb * 4 + 2 * c + b).wait_send()


def out_kernel(
    pool_ref, att_ref, w_pool, w_attn, out_ref,
    lhs, w_both, to_sib, from_sib, opp, to_right, to_left, opp_in, from_left, from_right,
    sib_send, sib_recv, opp_send, opp_recv, right_send, right_recv, left_send, left_recv,
):
    sp, tp, x, c = place()
    right = {"sp": sp, "tp": lax.rem(x + 1, 4) * 2 + c}
    left = {"sp": sp, "tp": lax.rem(x + 3, 4) * 2 + c}
    sib = {"sp": sp, "tp": x * 2 + 1 - c}
    meet([right, left, sib])
    w_both[pl.ds(0, 128), :] = w_pool[...]
    w_both[pl.ds(128, 128), :] = w_attn[...]
    lhs[:, 0:128] = pool_ref[...]
    lhs[:, 128:256] = turned(att_ref[...]).astype(BF16)
    order = (2, 1, 3, 0)

    def partial(offset, core):
        rows = pl.multiple_of((lax.rem(x + offset, 4) * 2 + core) * BLOCK, 32)
        return dot(lhs[pl.ds(rows, BLOCK), :], w_both[...])

    def sib_copy(k):
        return remote(to_sib.at[k], from_sib.at[k], sib_send.at[k], sib_recv.at[k], sib)

    for k, offset in enumerate(order):
        to_sib[k] = partial(offset, 1 - c).astype(BF16)
        sib_copy(k).start()

    def chip_sum(k):
        value = partial(order[k], c)
        sib_copy(k).wait_recv()
        return value + from_sib[k].astype(F32)

    first, second = pl.ds(0, HALF), pl.ds(HALF, HALF)
    opp[...] = chip_sum(0).astype(BF16)
    opp_copies = [
        remote(opp.at[first], opp_in.at[0], opp_send.at[0], opp_recv.at[0], right),
        remote(opp.at[second], opp_in.at[1], opp_send.at[1], opp_recv.at[1], left),
    ]
    for copy in opp_copies:
        copy.start()

    def near_copies(stage, landing, send, recv, device):
        return [remote(stage.at[rows], landing.at[rows], send.at[h], recv.at[h], device) for h, rows in enumerate((first, second))]

    rights = near_copies(to_right, from_left, right_send, right_recv, right)
    lefts = near_copies(to_left, from_right, left_send, left_recv, left)
    value_r = chip_sum(1)
    to_right[second, :] = value_r[HALF:].astype(BF16)
    rights[1].start()
    value_l = chip_sum(2)
    to_left[first, :] = value_l[:HALF].astype(BF16)
    lefts[0].start()
    opp_copies[0].wait_recv()
    to_right[first, :] = (value_r[:HALF] + opp_in[0].astype(F32)).astype(BF16)
    rights[0].start()
    opp_copies[1].wait_recv()
    to_left[second, :] = (value_l[HALF:] + opp_in[1].astype(F32)).astype(BF16)
    lefts[1].start()
    value = chip_sum(3)
    for copy in rights + lefts:
        copy.wait_recv()
    out_ref[...] = (value + from_left[...].astype(F32) + from_right[...].astype(F32)).astype(BF16)
    for copy in [sib_copy(k) for k in range(4)] + opp_copies + rights + lefts:
        copy.wait_send()


DMA = pltpu.SemaphoreType.DMA


def params(number):
    return pltpu.CompilerParams(collective_id=number, has_side_effects=True, vmem_limit_bytes=60 * 1024 * 1024)


def local(
    activations, in_gain, w_pool_in, pool_gain, w_qlat, w_kvlat, w_krope, qlat_gain, kvlat_gain,
    w_qup, w_kup, w_vup, qhead_gain, khead_gain, w_out_pool, w_out_attn,
):
    w_lat = jnp.concatenate([w_qlat, w_kvlat, w_krope], axis=1)
    tables = [jnp.asarray(t) for t in rotary_tables()]
    q_t, kv_t, pool_out = pl.pallas_call(
        front_kernel,
        name="front",
        out_shape=(
            jax.ShapeDtypeStruct((2, HEAD, ROWS), BF16),
            jax.ShapeDtypeStruct((2, LAT, ROWS), BF16),
            jax.ShapeDtypeStruct((ROWS, 128), BF16),
        ),
        in_specs=[VMEM_SPEC] * 16,
        out_specs=(VMEM_SPEC,) * 3,
        scratch_shapes=[
            pltpu.VMEM((8, BLOCK, D), BF16),
            pltpu.VMEM((ROWS, 192), F32),
            pltpu.VMEM((LAT, ROWS), BF16),
            pltpu.VMEM((8, LAT, ROWS), BF16),
            pltpu.VMEM((HALO + ROWS, 128), F32),
            pltpu.VMEM((HALO, 128), BF16),
            pltpu.VMEM((HALO, 128), BF16),
            pltpu.VMEM((192, QLAT), BF16),
            pltpu.VMEM((256, KVLAT), BF16),
            DMA((6,)), DMA((8,)), DMA((8, 2)),
            DMA((6,)), DMA((8,)), DMA((8, 2)),
            DMA((2,)),
        ],
        compiler_params=params(1),
    )(
        activations, in_gain[None, :], w_pool_in, w_lat, pool_gain[None, :], qlat_gain[:, None], kvlat_gain[:, None],
        w_qup, w_kup, w_vup, qhead_gain[:, None], khead_gain[:, None], *tables,
    )
    attended = pl.pallas_call(
        attend_kernel,
        name="attend",
        out_shape=jax.ShapeDtypeStruct((2, VDIM, ROWS), BF16),
        in_specs=[VMEM_SPEC] * 2,
        out_specs=VMEM_SPEC,
        scratch_shapes=[
            pltpu.VMEM((32, LAT, ROWS), BF16),
            pltpu.VMEM((32, ROWS, HEAD), BF16),
            pltpu.VMEM((2, HEAD, ROWS), BF16),
            pltpu.VMEM((2, VDIM, ROWS), F32),
            pltpu.VMEM((2, 8, ROWS), F32),
            pltpu.VMEM((2, VDIM, ROWS), BF16),
            pltpu.VMEM((2, VDIM, ROWS), BF16),
            DMA((2,)), DMA((32,)), DMA((2,)), DMA((2,)), DMA((2, 2, 4)), DMA((32,)), DMA((2,)), DMA((2,)),
        ],
        compiler_params=params(2),
    )(q_t, kv_t)
    return pl.pallas_call(
        out_kernel,
        name="output",
        out_shape=jax.ShapeDtypeStruct((BLOCK, D), BF16),
        in_specs=[VMEM_SPEC] * 4,
        out_specs=VMEM_SPEC,
        scratch_shapes=[
            pltpu.VMEM((ROWS, 256), BF16),
            pltpu.VMEM((256, D), BF16),
            pltpu.VMEM((4, BLOCK, D), BF16),
            pltpu.VMEM((4, BLOCK, D), BF16),
            pltpu.VMEM((BLOCK, D), BF16),
            pltpu.VMEM((BLOCK, D), BF16),
            pltpu.VMEM((BLOCK, D), BF16),
            pltpu.VMEM((2, HALF, D), BF16),
            pltpu.VMEM((BLOCK, D), BF16),
            pltpu.VMEM((BLOCK, D), BF16),
            DMA((4,)), DMA((4,)), DMA((2,)), DMA((2,)), DMA((2,)), DMA((2,)), DMA((2,)), DMA((2,)),
        ],
        compiler_params=params(3),
    )(pool_out, attended.reshape(2 * VDIM, ROWS), w_out_pool, w_out_attn)


def solution(mesh):
    placed = (
        P(("sp", "tp"), None), P(), P(None, "tp"), P("tp"), P(None, "tp"), P(None, "tp"), P(), P(), P(),
        P(None, "tp"), P(None, "tp"), P(None, "tp"), P(), P(), P("tp", None), P("tp", None),
    )
    return jax.shard_map(local, mesh=mesh, in_specs=placed, out_specs=P(("sp", "tp"), None), check_vma=False)
```

```python
import functools
import math

import jax
import jax.numpy as jnp
import numpy as np
from jax import lax
from jax.experimental import pallas as pl
from jax.experimental.pallas import tpu as pltpu
from jax.sharding import PartitionSpec as P

NOPE = 64
ROPE = 32
HEAD = NOPE + ROPE
VDIM = 64
QLAT = 768
KVLAT = 512
EPS = 1e-06
THETA = 10000.0
ROWS = 768
BLOCK = 96
HALF = BLOCK // 2
D = 2048
LAT = 160
HALO = 16
F32 = jnp.float32
BF16 = jnp.bfloat16
MESH = pl.DeviceIdType.MESH
VMEM_SPEC = pl.BlockSpec(memory_space=pltpu.VMEM)
SCALE = (1.0 / math.sqrt(HEAD)) * math.log2(math.e)


def dot(a, b):
    return jnp.dot(a, b, preferred_element_type=F32)


def turned(a):
    return jnp.transpose(a.astype(F32))


def column(row_ref):
    return jnp.transpose(jnp.broadcast_to(row_ref[...], (8, row_ref.shape[1])))[:, 0:1]


def rotary_tables():
    freq = THETA ** (-np.arange(0, ROPE, 2, dtype=np.float64) / ROPE)
    far = freq[:, None] * (np.arange(128, dtype=np.float64)[None, :] * ROWS)
    near = freq[:, None] * np.arange(ROWS, dtype=np.float64)[None, :]
    return tuple(t.astype(np.float32) for t in (np.cos(far), np.sin(far), np.cos(near), np.sin(near)))


def place():
    sp = lax.axis_index("sp")
    tp = lax.axis_index("tp")
    return sp, tp, tp // 2, lax.rem(tp, 2)


def meet(devices):
    barrier = pltpu.get_barrier_semaphore()
    for device in devices:
        pl.semaphore_signal(barrier, inc=1, device_id=device, device_id_type=MESH)
    pl.semaphore_wait(barrier, len(devices))


def remote(src, dst, send_sem, recv_sem, device):
    return pltpu.make_async_remote_copy(
        src_ref=src, dst_ref=dst, send_sem=send_sem, recv_sem=recv_sem, device_id=device, device_id_type=MESH
    )


class TpGather:
    def __init__(self, own, everything, half, sp, x, c, ring_send, sib_send, recv):
        self.own, self.all, self.half = own, everything, half
        self.x, self.c = x, c
        self.ring_send, self.sib_send, self.recv = ring_send, sib_send, recv
        self.right = {"sp": sp, "tp": lax.rem(x + 1, 4) * 2 + c}
        self.left = {"sp": sp, "tp": lax.rem(x + 3, 4) * 2 + c}
        self.sib = {"sp": sp, "tp": x * 2 + 1 - c}

    def index(self, offset, core):
        return lax.rem(self.x + 4 + offset, 4) * 2 + core

    def piece(self, idx, h):
        return self.all.at[idx, pl.ds(h * self.half, self.half)]

    def copy(self, src, idx, h, send, device):
        return remote(src, self.piece(idx, h), send, self.recv.at[idx, h], device)

    def start(self):
        me = self.index(0, self.c)
        for k, (device, h) in enumerate(((self.right, 0), (self.left, 1), (self.right, 1), (self.left, 0))):
            self.copy(self.own[h], me, h, self.ring_send.at[k], device).start()
        for h in range(2):
            self.copy(self.own[h], me, h, self.sib_send.at[h], self.sib).start()

    def wait_piece(self, idx, h):
        self.copy(self.own[h], idx, h, self.sib_send.at[0], self.sib).wait_recv()

    def got(self, offset, h, slot, onward=None, onward_slot=0):
        idx = self.index(offset, self.c)
        self.wait_piece(idx, h)
        if onward is not None:
            self.copy(self.piece(idx, h), idx, h, self.ring_send.at[onward_slot], onward).start()
        self.copy(self.piece(idx, h), idx, h, self.sib_send.at[slot], self.sib).start()

    def relay_first(self):
        self.got(-1, 0, 2, self.right, 4)
        self.got(1, 1, 3, self.left, 5)

    def relay_second(self):
        self.got(-1, 1, 4)
        self.got(1, 0, 5)

    def relay_far(self):
        self.got(2, 0, 6)
        self.got(2, 1, 7)

    def wait_sibling(self, offset):
        idx = self.index(offset, 1 - self.c)
        for h in range(2):
            self.wait_piece(idx, h)
        return idx

    def finish(self):
        for k in range(6):
            self.copy(self.own[0], 0, 0, self.ring_send.at[k], self.sib).wait_send()
        for k in range(8):
            self.copy(self.own[0], 0, 0, self.sib_send.at[k], self.sib).wait_send()


def front_kernel(
    act, in_gain, w_pool, w_qlat_t, w_kvlat_t, w_krope_t, pool_gain, q_gain, kv_gain, wq_t, w_kup, w_vup, qh_gain, kh_gain,
    far_cos, far_sin, near_cos, near_sin,
    q_out, kv_out, pool_out,
    act_all, lat_rows, lat_own, lat_all, pool_rows, halo_out, halo_in, w_lat, wkv_t,
    a_ring, a_sib, a_recv, l_ring, l_sib, l_recv, halo_sem,
):
    sp, tp, x, c = place()
    acts = TpGather([act.at[pl.ds(0, HALF)], act.at[pl.ds(HALF, HALF)]], act_all, HALF, sp, x, c, a_ring, a_sib, a_recv)
    lats = TpGather([lat_own.at[pl.ds(0, LAT // 2)], lat_own.at[pl.ds(LAT // 2, LAT // 2)]], lat_all, LAT // 2, sp, x, c, l_ring, l_sib, l_recv)
    behind = {"sp": lax.rem(sp + 1, 32), "tp": tp}
    before = {"sp": lax.rem(sp + 31, 32), "tp": tp}
    meet([acts.right, acts.left, acts.sib, behind, before])
    acts.start()

    def project(block, idx):
        rows = pl.multiple_of(idx * BLOCK, 32)
        value = block[...].astype(F32)
        factor = lax.rsqrt(jnp.mean(value * value, axis=1, keepdims=True) + EPS)
        normed = (value * factor * in_gain[...]).astype(BF16)
        pool_rows[pl.ds(HALO + rows, BLOCK), :] = dot(normed, w_pool[...]).astype(BF16).astype(F32)
        lat_rows[pl.ds(rows, BLOCK), :] = dot(normed, w_lat[...])

    w_lat[...] = turned(jnp.concatenate([w_qlat_t[...], w_kvlat_t[...], w_krope_t[...]], axis=0)).astype(BF16)
    project(act, tp)
    wkv_t[pl.ds(0, 128), :] = turned(w_kup[...]).astype(BF16)
    wkv_t[pl.ds(128, 128), :] = turned(w_vup[...]).astype(BF16)
    idx = acts.wait_sibling(0)
    project(act_all.at[idx], idx)
    acts.relay_first()
    acts.relay_second()
    for offset in (-1, 1):
        idx = acts.index(offset, c)
        project(act_all.at[idx], idx)
    for offset in (-1, 1):
        idx = acts.wait_sibling(offset)
        project(act_all.at[idx], idx)
    acts.relay_far()
    idx = acts.index(2, c)
    project(act_all.at[idx], idx)
    idx = acts.wait_sibling(2)
    project(act_all.at[idx], idx)

    lat_t = jnp.transpose(lat_rows[...])
    lat_own[...] = lat_t[:LAT].astype(BF16)
    rope_t = lat_t[LAT:].astype(BF16).astype(F32)
    halo_out[...] = pool_rows[pl.ds(ROWS, HALO), :].astype(BF16)
    lats.start()
    halo = remote(halo_out, halo_in, halo_sem.at[0], halo_sem.at[1], behind)
    halo.start()
    lat_all[tp] = lat_own[...]

    cos = jnp.sum(jnp.where(lax.broadcasted_iota(jnp.int32, (16, 128), 1) == sp, far_cos[...], 0.0), axis=1, keepdims=True)
    sin = jnp.sum(jnp.where(lax.broadcasted_iota(jnp.int32, (16, 128), 1) == sp, far_sin[...], 0.0), axis=1, keepdims=True)
    cosine = cos * near_cos[...] - sin * near_sin[...]
    sine = sin * near_cos[...] + cos * near_sin[...]

    halo.wait_recv()
    pool_rows[pl.ds(0, HALO), :] = jnp.where(sp > 0, halo_in[...].astype(F32), 0.0)
    window = jnp.left_shift(jnp.int32(2), tp // 2)
    total = jnp.zeros((ROWS, 128), F32)
    for lag in range(16):
        total = total + jnp.where(lag < window, pool_rows[pl.ds(HALO - lag, ROWS), :], 0.0)
    position = sp * ROWS + lax.broadcasted_iota(jnp.int32, (ROWS, 128), 0)
    divisor = jnp.minimum(position + 1, window).astype(F32)
    pooled = total / divisor - pool_rows[pl.ds(HALO, ROWS), :]
    pool_out[...] = (pooled * pool_gain[...]).astype(BF16)

    lats.relay_first()
    lats.relay_second()
    lats.relay_far()
    for offset in (0, -1, 1, 2):
        lats.wait_sibling(offset)

    q_lat = lat_all[:, 0:96, :].reshape(QLAT, ROWS).astype(F32)
    q_norm = q_lat * lax.rsqrt(jnp.sum(q_lat * q_lat, axis=0, keepdims=True) / QLAT + EPS) * column(q_gain)
    raw = dot(wq_t[...], q_norm.astype(BF16)).astype(BF16).astype(F32)
    kv_lat = lat_all[:, 96:LAT, :].reshape(KVLAT, ROWS).astype(F32)
    kv_norm = kv_lat * lax.rsqrt(jnp.sum(kv_lat * kv_lat, axis=0, keepdims=True) / KVLAT + EPS) * column(kv_gain)
    plain = dot(wkv_t[...], kv_norm.astype(BF16)).astype(BF16)

    def finish(head, gain):
        factor = lax.rsqrt(jnp.sum(head * head, axis=0, keepdims=True) / HEAD + EPS)
        head = head * factor * gain
        lower, upper = head[64:80], head[80:96]
        return jnp.concatenate([head[:64], lower * cosine - upper * sine, upper * cosine + lower * sine], axis=0)

    for h in range(2):
        q_out[h] = (finish(raw[h * 96 : h * 96 + 96], column(qh_gain)) * SCALE).astype(BF16)
        joined = jnp.concatenate([plain[h * 64 : h * 64 + 64].astype(F32), rope_t], axis=0)
        kv_out[h, 0:96, :] = finish(joined, column(kh_gain)).astype(BF16)
        kv_out[h, 96:160, :] = plain[128 + h * 64 : 192 + h * 64]
    acts.finish()
    lats.finish()
    halo.wait_send()


def attend_kernel(
    q_ref, kv_ref, pool_ref, w_pool, w_attn, out_ref,
    kv_all, k_rows, q_in, acc, den, o_rows, att_all, pool_in, w_all, lhs,
    c_send, kv_recv, q_send, q_recv, ring_send, sib_send, o_send, o_recv, p_send, p_recv, w_ring, w_sib, w_recv,
):
    sp, tp, x, c = place()
    z, y = sp // 4, lax.rem(sp, 4)
    even = lax.rem(y, 2) == 0
    owner = y // 2
    part = lax.rem(y, 2)
    q_z = jnp.where(even, z, 7 - z)
    q_c = jnp.where(even, owner, (3 - y) // 2)

    def device(yy, zz, cc, xx=x):
        return {"sp": zz * 4 + yy, "tp": xx * 2 + cc}

    up = device(y, lax.rem(z + 1, 8), c)
    down = device(y, lax.rem(z + 7, 8), c)
    sib = device(y, z, 1 - c)
    weights_out = TpGather([w_pool, w_attn], w_all, 128, sp, x, c, w_ring, w_sib, w_recv)

    friends = [up, down]
    for dy in range(4):
        for dc in range(2):
            yy, cc = lax.rem(y + dy, 4), lax.rem(c + dc, 2)
            friends.append(device(yy, 7 - z, cc))
            if dy or dc:
                friends.append(device(yy, z, cc))
    friends += [{"sp": sp, "tp": lax.rem(tp + k, 8)} for k in range(1, 8)]
    for dx in range(1, 4):
        for dy in range(4):
            friends.append(device(lax.rem(y + dy, 4), q_z, q_c, lax.rem(x + dx, 4)))
    meet(friends)

    def kv_copy(j):
        return remote(kv_ref.at[j], kv_all.at[sp], c_send.at[j], kv_recv.at[sp], device(2 * c + j, z, owner))

    def q_copy(j):
        return remote(q_ref.at[j], q_in.at[part], q_send.at[j], q_recv.at[part], device(2 * c + j, q_z, q_c))

    for j in range(2):
        here = 2 * c + j == y

        @pl.when(jnp.logical_not(here))
        def _():
            kv_copy(j).start()

        @pl.when(here)
        def _():
            kv_all[sp] = kv_ref[j]

    for j in range(2):
        here = jnp.logical_and(even, 2 * c + j == y)

        @pl.when(jnp.logical_not(here))
        def _():
            q_copy(j).start()

        @pl.when(here)
        def _():
            q_in[0] = q_ref[j]

    weights_out.start()

    def pool_copy(k):
        to = lax.rem(tp + k, 8)
        rows = pl.multiple_of(to * BLOCK, 32)
        return remote(pool_ref.at[pl.ds(rows, BLOCK)], pool_in.at[tp], p_send.at[k], p_recv.at[tp], {"sp": sp, "tp": to})

    for k in range(1, 8):
        pool_copy(k).start()
    pool_in[tp] = pool_ref[pl.ds(pl.multiple_of(tp * BLOCK, 32), BLOCK), :]
    w_all[tp, pl.ds(0, 128), :] = w_pool[...]
    w_all[tp, pl.ds(128, 128), :] = w_attn[...]
    acc[...] = jnp.zeros_like(acc)
    den[...] = jnp.zeros_like(den)

    def wait_slot(slot):
        remote(kv_all.at[slot], kv_all.at[slot], sib_send.at[slot], kv_recv.at[slot], sib).wait_recv()

    def ring_copy(slot, way, b, s):
        return remote(kv_all.at[slot], kv_all.at[slot], ring_send.at[way, b, s], kv_recv.at[slot], (up, down)[way])

    def sib_copy(slot):
        return remote(kv_all.at[slot], kv_all.at[slot], sib_send.at[slot], kv_recv.at[slot], sib)

    def attend(slots, qb, diagonal):
        for qc in range(3):
            columns = pl.ds(qc * 256, 256)
            keys = (qc + 1) * 256 if diagonal else ROWS
            for slot in slots:
                scores = dot(k_rows[slot, pl.ds(0, keys), :], q_in[qb, :, columns])
                weights = jnp.exp2(scores)
                if diagonal:
                    k_pos = lax.broadcasted_iota(jnp.int32, (keys, 256), 0)
                    q_pos = lax.broadcasted_iota(jnp.int32, (keys, 256), 1) + qc * 256
                    weights = jnp.where(k_pos <= q_pos, weights, 0.0)
                den[qb, :, columns] += jnp.sum(weights.reshape(keys // 8, 8, 256), axis=0)
                acc[qb, :, columns] += dot(kv_all[slot, pl.ds(96, 64), pl.ds(0, keys)], weights.astype(BF16))

    q_plane = (z, 7 - z)
    q_row = (2 * c, 3 - 2 * c)

    def plane_of(way, s):
        return lax.rem(z + 8 - s, 8) if way == 0 else lax.rem(z + s, 8)

    def pass_on(s, b):
        @pl.when(jnp.logical_and(s == 0, 2 * c + b != y))
        def _():
            wait_slot(z * 4 + 2 * c + b)

        for way in ((0, 1), (1, 0))[b]:
            limit = 4 if way == b else 3
            slot = plane_of(way, s) * 4 + 2 * c + b

            @pl.when(jnp.logical_and(s >= 1, s <= limit))
            def _():
                wait_slot(slot)

            @pl.when(s < limit)
            def _():
                ring_copy(slot, way, b, s).start()

            @pl.when(jnp.logical_and(jnp.logical_or(s >= 1, way == 0), s <= limit))
            def _():
                sib_copy(slot).start()

    def use(zb):
        first = zb * 4
        for b in range(2):
            wait_slot(first + 2 * (1 - c) + b)

        @pl.when(zb <= jnp.maximum(z, 7 - z))
        def _():
            for yb in range(4):
                k_rows[first + yb] = turned(kv_all[first + yb, pl.ds(0, HEAD), :]).astype(BF16)

        @pl.loop(0, 2)
        def _(qb):
            plane = jnp.where(qb == 0, q_plane[0], q_plane[1])
            row = jnp.where(qb == 0, q_row[0], q_row[1])

            @pl.when(zb < plane)
            def _():
                attend([first + yb for yb in range(4)], qb, False)

            @pl.when(zb == plane)
            def _():
                @pl.loop(0, row)
                def _(yb):
                    attend([first + yb], qb, False)

                attend([first + row], qb, True)

    @pl.loop(0, 10)
    def _(turn):
        s, b = turn // 2, lax.rem(turn, 2)
        for k in range(2):
            @pl.when(b == k)
            def _():
                pass_on(s, k)

        @pl.when(jnp.logical_and(turn == 1, 2 * c != y))
        def _():
            remote(q_ref.at[0], q_in.at[0], q_send.at[0], q_recv.at[0], sib).wait_recv()

        @pl.when(turn == 1)
        def _():
            remote(q_ref.at[0], q_in.at[1], q_send.at[0], q_recv.at[1], sib).wait_recv()

        @pl.when(turn == 4)
        def _():
            weights_out.relay_first()

        @pl.when(turn == 6)
        def _():
            weights_out.relay_second()

        @pl.when(turn == 8)
        def _():
            weights_out.relay_far()

        done = s - 1
        zb = lax.rem(z + 8 + jnp.where(b == 0, -done, done), 8)

        @pl.when(jnp.logical_and(turn >= 2, turn != 3))
        def _():
            use(zb)

    use(lax.rem(z + 4, 8))

    def back(qb, t):
        to_y, to_z = (2 * c, z) if qb == 0 else (3 - 2 * c, 7 - z)
        return remote(
            o_rows.at[qb, pl.ds(t * BLOCK, BLOCK)], att_all.at[4 * x + y], o_send.at[qb, t], o_recv.at[4 * x + y],
            {"sp": to_z * 4 + to_y, "tp": t},
        )

    mine = jnp.logical_and(even, 2 * c == y)

    def is_me(qb, t):
        return jnp.logical_and(2 * c == y, tp == t) if qb == 0 else False

    for qb in (1, 0):
        o_rows[qb] = jnp.transpose(acc[qb] / jnp.sum(den[qb], axis=0, keepdims=True)).astype(BF16)
        for t in range(8):
            if qb == 1:
                back(qb, t).start()
            else:
                @pl.when(jnp.logical_not(is_me(qb, t)))
                def _():
                    back(qb, t).start()

                @pl.when(is_me(qb, t))
                def _():
                    att_all[4 * x + y] = o_rows[0, pl.ds(t * BLOCK, BLOCK), :]

    for k in range(1, 8):
        idx = lax.rem(tp + k, 8)
        remote(pool_in.at[0], pool_in.at[idx], p_send.at[k], p_recv.at[idx], sib).wait_recv()
    for offset in (0, -1, 1, 2):
        weights_out.wait_sibling(offset)
    for t in range(8):
        lhs[:, pl.ds(t * 256, 128)] = pool_in[t]

    @pl.loop(0, 16)
    def _(head):
        @pl.when(jnp.logical_not(jnp.logical_and(mine, head == 4 * x + y)))
        def _():
            remote(att_all.at[0], att_all.at[head], o_send.at[0, 0], o_recv.at[head], sib).wait_recv()

    for t in range(8):
        lhs[:, pl.ds(t * 256 + 128, 128)] = jnp.concatenate([att_all[2 * t], att_all[2 * t + 1]], axis=1)
    for part_of in range(4):
        columns = pl.ds(part_of * 512, 512)
        out_ref[:, columns] = dot(lhs[...], w_all[:, :, columns].reshape(D, 512)).astype(BF16)

    for j in range(2):
        @pl.when(jnp.logical_not(jnp.logical_and(even, 2 * c + j == y)))
        def _():
            q_copy(j).wait_send()

        @pl.when(2 * c + j != y)
        def _():
            kv_copy(j).wait_send()

    for t in range(8):
        back(1, t).wait_send()

        @pl.when(jnp.logical_not(is_me(0, t)))
        def _():
            back(0, t).wait_send()

    for k in range(1, 8):
        pool_copy(k).wait_send()
    weights_out.finish()
    for b in range(2):
        for way in range(2):
            for s in range(4 if way == b else 3):
                ring_copy(0, way, b, s).wait_send()

    @pl.loop(0, 8)
    def _(zb):
        for b in range(2):
            sib_copy(zb * 4 + 2 * c + b).wait_send()


DMA = pltpu.SemaphoreType.DMA


def params(number):
    return pltpu.CompilerParams(collective_id=number, has_side_effects=True, vmem_limit_bytes=60 * 1024 * 1024)


def local(
    activations, in_gain, w_pool_in, pool_gain, w_qlat, w_kvlat, w_krope, qlat_gain, kvlat_gain,
    w_qup, w_kup, w_vup, qhead_gain, khead_gain, w_out_pool, w_out_attn,
):
    tables = [jnp.asarray(t) for t in rotary_tables()]
    q_t, kv_t, pool_out = pl.pallas_call(
        front_kernel,
        name="front",
        out_shape=(
            jax.ShapeDtypeStruct((2, HEAD, ROWS), BF16),
            jax.ShapeDtypeStruct((2, LAT, ROWS), BF16),
            jax.ShapeDtypeStruct((ROWS, 128), BF16),
        ),
        in_specs=[VMEM_SPEC] * 18,
        out_specs=(VMEM_SPEC,) * 3,
        scratch_shapes=[
            pltpu.VMEM((8, BLOCK, D), BF16),
            pltpu.VMEM((ROWS, 192), F32),
            pltpu.VMEM((LAT, ROWS), BF16),
            pltpu.VMEM((8, LAT, ROWS), BF16),
            pltpu.VMEM((HALO + ROWS, 128), F32),
            pltpu.VMEM((HALO, 128), BF16),
            pltpu.VMEM((HALO, 128), BF16),
            pltpu.VMEM((D, 192), BF16),
            pltpu.VMEM((256, KVLAT), BF16),
            DMA((6,)), DMA((8,)), DMA((8, 2)),
            DMA((6,)), DMA((8,)), DMA((8, 2)),
            DMA((2,)),
        ],
        compiler_params=params(1),
    )(
        activations, in_gain[None, :], w_pool_in, w_qlat.T, w_kvlat.T, w_krope.T, pool_gain[None, :], qlat_gain[None, :],
        kvlat_gain[None, :], w_qup.T, w_kup, w_vup, qhead_gain[None, :], khead_gain[None, :], *tables,
    )
    return pl.pallas_call(
        attend_kernel,
        name="attend",
        out_shape=jax.ShapeDtypeStruct((BLOCK, D), BF16),
        in_specs=[VMEM_SPEC] * 5,
        out_specs=VMEM_SPEC,
        scratch_shapes=[
            pltpu.VMEM((32, LAT, ROWS), BF16),
            pltpu.VMEM((32, ROWS, HEAD), BF16),
            pltpu.VMEM((2, HEAD, ROWS), BF16),
            pltpu.VMEM((2, VDIM, ROWS), F32),
            pltpu.VMEM((2, 8, ROWS), F32),
            pltpu.VMEM((2, ROWS, VDIM), BF16),
            pltpu.VMEM((16, BLOCK, VDIM), BF16),
            pltpu.VMEM((8, BLOCK, 128), BF16),
            pltpu.VMEM((8, 256, D), BF16),
            pltpu.VMEM((BLOCK, D), BF16),
            DMA((2,)), DMA((32,)), DMA((2,)), DMA((2,)), DMA((2, 2, 4)), DMA((32,)), DMA((2, 8)), DMA((16,)),
            DMA((8,)), DMA((8,)), DMA((6,)), DMA((8,)), DMA((8, 2)),
        ],
        compiler_params=params(2),
    )(q_t, kv_t, pool_out, w_out_pool, w_out_attn)


def solution(mesh):
    placed = (
        P(("sp", "tp"), None), P(), P(None, "tp"), P("tp"), P(None, "tp"), P(None, "tp"), P(), P(), P(),
        P(None, "tp"), P(None, "tp"), P(None, "tp"), P(), P(), P("tp", None), P("tp", None),
    )
    return jax.shard_map(local, mesh=mesh, in_specs=placed, out_specs=P(("sp", "tp"), None), check_vma=False)
```

```python
import functools
import math

import jax
import jax.numpy as jnp
import numpy as np
from jax import lax
from jax.experimental import pallas as pl
from jax.experimental.pallas import tpu as pltpu
from jax.sharding import PartitionSpec as P

NOPE = 64
ROPE = 32
HEAD = NOPE + ROPE
VDIM = 64
QLAT = 768
KVLAT = 512
EPS = 1e-06
THETA = 10000.0
ROWS = 768
BLOCK = 96
HALF = BLOCK // 2
D = 2048
LAT = 160
HALO = 16
F32 = jnp.float32
BF16 = jnp.bfloat16
MESH = pl.DeviceIdType.MESH
VMEM_SPEC = pl.BlockSpec(memory_space=pltpu.VMEM)
SCALE = (1.0 / math.sqrt(HEAD)) * math.log2(math.e)


def dot(a, b):
    return jnp.dot(a, b, preferred_element_type=F32)


def turned(a):
    return jnp.transpose(a.astype(F32))


def column(row_ref):
    return jnp.transpose(jnp.broadcast_to(row_ref[...], (8, row_ref.shape[1])))[:, 0:1]


def rotary_tables():
    freq = THETA ** (-np.arange(0, ROPE, 2, dtype=np.float64) / ROPE)
    far = freq[:, None] * (np.arange(128, dtype=np.float64)[None, :] * ROWS)
    near = freq[:, None] * np.arange(ROWS, dtype=np.float64)[None, :]
    return tuple(t.astype(np.float32) for t in (np.cos(far), np.sin(far), np.cos(near), np.sin(near)))


def place():
    sp = lax.axis_index("sp")
    tp = lax.axis_index("tp")
    return sp, tp, tp // 2, lax.rem(tp, 2)


def meet(devices):
    barrier = pltpu.get_barrier_semaphore()
    for device in devices:
        pl.semaphore_signal(barrier, inc=1, device_id=device, device_id_type=MESH)
    pl.semaphore_wait(barrier, len(devices))


def remote(src, dst, send_sem, recv_sem, device):
    return pltpu.make_async_remote_copy(
        src_ref=src, dst_ref=dst, send_sem=send_sem, recv_sem=recv_sem, device_id=device, device_id_type=MESH
    )


class TpGather:
    def __init__(self, own, everything, half, sp, x, c, ring_send, sib_send, recv):
        self.own, self.all, self.half = own, everything, half
        self.x, self.c = x, c
        self.ring_send, self.sib_send, self.recv = ring_send, sib_send, recv
        self.right = {"sp": sp, "tp": lax.rem(x + 1, 4) * 2 + c}
        self.left = {"sp": sp, "tp": lax.rem(x + 3, 4) * 2 + c}
        self.sib = {"sp": sp, "tp": x * 2 + 1 - c}

    def index(self, offset, core):
        return lax.rem(self.x + 4 + offset, 4) * 2 + core

    def piece(self, idx, h):
        return self.all.at[idx, pl.ds(h * self.half, self.half)]

    def copy(self, src, idx, h, send, device):
        return remote(src, self.piece(idx, h), send, self.recv.at[idx, h], device)

    def start(self):
        me = self.index(0, self.c)
        for k, (device, h) in enumerate(((self.right, 0), (self.left, 1), (self.right, 1), (self.left, 0))):
            self.copy(self.own[h], me, h, self.ring_send.at[k], device).start()
        for h in range(2):
            self.copy(self.own[h], me, h, self.sib_send.at[h], self.sib).start()

    def wait_piece(self, idx, h):
        self.copy(self.own[h], idx, h, self.sib_send.at[0], self.sib).wait_recv()

    def got(self, offset, h, slot, onward=None, onward_slot=0):
        idx = self.index(offset, self.c)
        self.wait_piece(idx, h)
        if onward is not None:
            self.copy(self.piece(idx, h), idx, h, self.ring_send.at[onward_slot], onward).start()
        self.copy(self.piece(idx, h), idx, h, self.sib_send.at[slot], self.sib).start()

    def relay_first(self):
        self.got(-1, 0, 2, self.right, 4)
        self.got(1, 1, 3, self.left, 5)

    def relay_second(self):
        self.got(-1, 1, 4)
        self.got(1, 0, 5)

    def relay_far(self):
        self.got(2, 0, 6)
        self.got(2, 1, 7)

    def wait_sibling(self, offset):
        idx = self.index(offset, 1 - self.c)
        for h in range(2):
            self.wait_piece(idx, h)
        return idx

    def finish(self):
        for k in range(6):
            self.copy(self.own[0], 0, 0, self.ring_send.at[k], self.sib).wait_send()
        for k in range(8):
            self.copy(self.own[0], 0, 0, self.sib_send.at[k], self.sib).wait_send()


def mixer_kernel(
    act, in_gain, w_pool, w_qlat_t, w_kvlat_t, w_krope_t, pool_gain, q_gain, kv_gain, wq_t, w_kup, w_vup, qh_gain, kh_gain,
    far_cos, far_sin, near_cos, near_sin, w_out_pool, w_out_attn,
    out_ref,
    act_all, lat_rows, kvl_own, kvl_all, ql_own, ql_all, pool_rows, halo_out, halo_in, w_lat, wkv_t, q_own, kv_own, pool_own,
    kv_all, k_rows, q_in, acc, den, o_rows, att_all, pool_in, w_all, lhs, total,
    a_ring, a_sib, a_recv, k_ring, k_sib, k_recv, l_ring, l_sib, l_recv, halo_sem,
    c_send, kv_recv, q_send, q_recv, ring_send, sib_send, o_send, o_recv, p_send, p_recv, w_ring, w_sib, w_recv,
):
    sp, tp, x, c = place()
    z, y = sp // 4, lax.rem(sp, 4)
    even = lax.rem(y, 2) == 0
    owner = y // 2
    part = lax.rem(y, 2)
    q_z = jnp.where(even, z, 7 - z)
    q_c = jnp.where(even, owner, (3 - y) // 2)

    def device(yy, zz, cc, xx=x):
        return {"sp": zz * 4 + yy, "tp": xx * 2 + cc}

    up = device(y, lax.rem(z + 1, 8), c)
    down = device(y, lax.rem(z + 7, 8), c)
    sib = device(y, z, 1 - c)
    behind = {"sp": lax.rem(sp + 1, 32), "tp": tp}
    before = {"sp": lax.rem(sp + 31, 32), "tp": tp}

    def gather(own, everything, half, *sems):
        return TpGather(own, everything, half, sp, x, c, *sems)

    acts = gather([act.at[pl.ds(0, HALF)], act.at[pl.ds(HALF, HALF)]], act_all, HALF, a_ring, a_sib, a_recv)
    kv_lats = gather([kvl_own.at[pl.ds(0, 32)], kvl_own.at[pl.ds(32, 32)]], kvl_all, 32, k_ring, k_sib, k_recv)
    q_lats = gather([ql_own.at[pl.ds(0, 48)], ql_own.at[pl.ds(48, 48)]], ql_all, 48, l_ring, l_sib, l_recv)
    weights_out = gather([w_out_pool, w_out_attn], w_all, 128, w_ring, w_sib, w_recv)

    friends = [up, down, behind, before]
    for dy in range(4):
        for dc in range(2):
            yy, cc = lax.rem(y + dy, 4), lax.rem(c + dc, 2)
            friends.append(device(yy, 7 - z, cc))
            if dy or dc:
                friends.append(device(yy, z, cc))
    friends += [{"sp": sp, "tp": lax.rem(tp + k, 8)} for k in range(1, 8)]
    for dx in range(1, 4):
        for dy in range(4):
            friends.append(device(lax.rem(y + dy, 4), q_z, q_c, lax.rem(x + dx, 4)))
    meet(friends)

    acts.start()

    def project(block, idx):
        rows = pl.multiple_of(idx * BLOCK, 32)
        value = block[...].astype(F32)
        factor = lax.rsqrt(jnp.mean(value * value, axis=1, keepdims=True) + EPS)
        normed = (value * factor * in_gain[...]).astype(BF16)
        pool_rows[pl.ds(HALO + rows, BLOCK), :] = dot(normed, w_pool[...]).astype(BF16).astype(F32)
        lat_rows[pl.ds(rows, BLOCK), :] = dot(normed, w_lat[...])

    w_lat[...] = turned(jnp.concatenate([w_qlat_t[...], w_kvlat_t[...], w_krope_t[...]], axis=0)).astype(BF16)
    project(act, tp)
    wkv_t[pl.ds(0, 128), :] = turned(w_kup[...]).astype(BF16)
    wkv_t[pl.ds(128, 128), :] = turned(w_vup[...]).astype(BF16)
    idx = acts.wait_sibling(0)
    project(act_all.at[idx], idx)
    acts.relay_first()
    acts.relay_second()
    for offset in (-1, 1):
        idx = acts.index(offset, c)
        project(act_all.at[idx], idx)
    for offset in (-1, 1):
        idx = acts.wait_sibling(offset)
        project(act_all.at[idx], idx)
    acts.relay_far()
    idx = acts.index(2, c)
    project(act_all.at[idx], idx)
    idx = acts.wait_sibling(2)
    project(act_all.at[idx], idx)

    lat_t = jnp.transpose(lat_rows[...])
    kvl_own[...] = lat_t[96:160].astype(BF16)
    ql_own[...] = lat_t[0:96].astype(BF16)
    rope_t = lat_t[160:192].astype(BF16).astype(F32)
    halo_out[...] = pool_rows[pl.ds(ROWS, HALO), :].astype(BF16)
    kv_lats.start()
    halo = remote(halo_out, halo_in, halo_sem.at[0], halo_sem.at[1], behind)
    halo.start()
    kvl_all[tp] = kvl_own[...]
    ql_all[tp] = ql_own[...]

    column_of = lax.broadcasted_iota(jnp.int32, (16, 128), 1) == sp
    cos = jnp.sum(jnp.where(column_of, far_cos[...], 0.0), axis=1, keepdims=True)
    sin = jnp.sum(jnp.where(column_of, far_sin[...], 0.0), axis=1, keepdims=True)
    cosine = cos * near_cos[...] - sin * near_sin[...]
    sine = sin * near_cos[...] + cos * near_sin[...]

    kv_lats.relay_first()
    q_lats.start()
    kv_lats.relay_second()
    kv_lats.relay_far()
    for offset in (0, -1, 1, 2):
        kv_lats.wait_sibling(offset)

    def finish(head, gain):
        factor = lax.rsqrt(jnp.sum(head * head, axis=0, keepdims=True) / HEAD + EPS)
        head = head * factor * gain
        lower, upper = head[64:80], head[80:96]
        return jnp.concatenate([head[:64], lower * cosine - upper * sine, upper * cosine + lower * sine], axis=0)

    kv_lat = kvl_all[...].reshape(KVLAT, ROWS).astype(F32)
    kv_norm = kv_lat * lax.rsqrt(jnp.sum(kv_lat * kv_lat, axis=0, keepdims=True) / KVLAT + EPS) * column(kv_gain)
    plain = dot(wkv_t[...], kv_norm.astype(BF16)).astype(BF16)
    for h in range(2):
        joined = jnp.concatenate([plain[h * 64 : h * 64 + 64].astype(F32), rope_t], axis=0)
        kv_own[h, 0:96, :] = finish(joined, column(kh_gain)).astype(BF16)
        kv_own[h, 96:160, :] = plain[128 + h * 64 : 192 + h * 64]

    def kv_copy(j):
        return remote(kv_own.at[j], kv_all.at[sp], c_send.at[j], kv_recv.at[sp], device(2 * c + j, z, owner))

    def q_copy(j):
        return remote(q_own.at[j], q_in.at[part], q_send.at[j], q_recv.at[part], device(2 * c + j, q_z, q_c))

    for j in range(2):
        here = 2 * c + j == y

        @pl.when(jnp.logical_not(here))
        def _():
            kv_copy(j).start()

        @pl.when(here)
        def _():
            kv_all[sp] = kv_own[j]

    q_lats.relay_first()
    q_lats.relay_second()
    q_lats.relay_far()
    for offset in (0, -1, 1, 2):
        q_lats.wait_sibling(offset)
    weights_out.start()
    q_lat = ql_all[...].reshape(QLAT, ROWS).astype(F32)
    q_norm = q_lat * lax.rsqrt(jnp.sum(q_lat * q_lat, axis=0, keepdims=True) / QLAT + EPS) * column(q_gain)
    raw = dot(wq_t[...], q_norm.astype(BF16)).astype(BF16).astype(F32)
    for h in range(2):
        q_own[h] = (finish(raw[h * 96 : h * 96 + 96], column(qh_gain)) * SCALE).astype(BF16)

    for j in range(2):
        here = jnp.logical_and(even, 2 * c + j == y)

        @pl.when(jnp.logical_not(here))
        def _():
            q_copy(j).start()

        @pl.when(here)
        def _():
            q_in[0] = q_own[j]

    def wait_slot(slot):
        remote(kv_all.at[slot], kv_all.at[slot], sib_send.at[slot], kv_recv.at[slot], sib).wait_recv()

    def ring_copy(slot, way, b, s):
        return remote(kv_all.at[slot], kv_all.at[slot], ring_send.at[way, b, s], kv_recv.at[slot], (up, down)[way])

    def sib_copy(slot):
        return remote(kv_all.at[slot], kv_all.at[slot], sib_send.at[slot], kv_recv.at[slot], sib)

    def pool_copy(k):
        to = lax.rem(tp + k, 8)
        rows = pl.multiple_of(to * BLOCK, 32)
        return remote(pool_own.at[pl.ds(rows, BLOCK)], pool_in.at[tp], p_send.at[k], p_recv.at[tp], {"sp": sp, "tp": to})

    def mix_pool():
        halo.wait_recv()
        pool_rows[pl.ds(0, HALO), :] = jnp.where(sp > 0, halo_in[...].astype(F32), 0.0)
        window = jnp.left_shift(jnp.int32(2), tp // 2)
        summed = jnp.zeros((ROWS, 128), F32)
        for lag in range(16):
            summed = summed + jnp.where(lag < window, pool_rows[pl.ds(HALO - lag, ROWS), :], 0.0)
        position = sp * ROWS + lax.broadcasted_iota(jnp.int32, (ROWS, 128), 0)
        divisor = jnp.minimum(position + 1, window).astype(F32)
        pooled = summed / divisor - pool_rows[pl.ds(HALO, ROWS), :]
        pool_own[...] = (pooled * pool_gain[...]).astype(BF16)
        for k in range(1, 8):
            pool_copy(k).start()
        pool_in[tp] = pool_own[pl.ds(pl.multiple_of(tp * BLOCK, 32), BLOCK), :]
        w_all[tp, pl.ds(0, 128), :] = w_out_pool[...]
        w_all[tp, pl.ds(128, 128), :] = w_out_attn[...]
        acc[...] = jnp.zeros_like(acc)
        den[...] = jnp.zeros_like(den)

    def attend(slots, qb, diagonal):
        for qc in range(3):
            columns = pl.ds(qc * 256, 256)
            keys = (qc + 1) * 256 if diagonal else ROWS
            for slot in slots:
                scores = dot(k_rows[slot, pl.ds(0, keys), :], q_in[qb, :, columns])
                weights = jnp.exp2(scores)
                if diagonal:
                    k_pos = lax.broadcasted_iota(jnp.int32, (keys, 256), 0)
                    q_pos = lax.broadcasted_iota(jnp.int32, (keys, 256), 1) + qc * 256
                    weights = jnp.where(k_pos <= q_pos, weights, 0.0)
                den[qb, :, columns] += jnp.sum(weights.reshape(keys // 8, 8, 256), axis=0)
                acc[qb, :, columns] += dot(kv_all[slot, pl.ds(96, 64), pl.ds(0, keys)], weights.astype(BF16))

    def plane_of(way, s):
        return lax.rem(z + 8 - s, 8) if way == 0 else lax.rem(z + s, 8)

    def pass_on(s, b):
        @pl.when(jnp.logical_and(s == 0, 2 * c + b != y))
        def _():
            wait_slot(z * 4 + 2 * c + b)

        for way in ((0, 1), (1, 0))[b]:
            limit = 4 if way == b else 3
            slot = plane_of(way, s) * 4 + 2 * c + b

            @pl.when(jnp.logical_and(s >= 1, s <= limit))
            def _():
                wait_slot(slot)

            @pl.when(s < limit)
            def _():
                ring_copy(slot, way, b, s).start()

            @pl.when(jnp.logical_and(jnp.logical_or(s >= 1, way == 0), s <= limit))
            def _():
                sib_copy(slot).start()

    def query_block(qb):
        return jnp.where(qb == 0, z, 7 - z), jnp.where(qb == 0, 2 * c, 3 - 2 * c)

    def unpack(zb):
        first = zb * 4
        for b in range(2):
            wait_slot(first + 2 * (1 - c) + b)

        @pl.when(zb <= jnp.maximum(z, 7 - z))
        def _():
            for yb in range(4):
                k_rows[first + yb] = turned(kv_all[first + yb, pl.ds(0, HEAD), :]).astype(BF16)

    def use(zb, qb):
        first = zb * 4
        plane, row = query_block(qb)

        @pl.when(zb < plane)
        def _():
            attend([first + yb for yb in range(4)], qb, False)

        @pl.when(zb == plane)
        def _():
            @pl.loop(0, row)
            def _(yb):
                attend([first + yb], qb, False)

            attend([first + row], qb, True)

    def back(qb, t):
        to_z, to_y = query_block(qb)
        return remote(
            o_rows.at[qb, t], att_all.at[4 * x + y], o_send.at[qb, t], o_recv.at[4 * x + y],
            {"sp": to_z * 4 + to_y, "tp": t},
        )

    def is_me(qb, t):
        return jnp.logical_and(jnp.logical_and(qb == 0, 2 * c == y), tp == t)

    def send_back(qb):
        rows = jnp.transpose(acc[qb] / jnp.sum(den[qb], axis=0, keepdims=True)).reshape(8, 2, HALF, VDIM)
        o_rows[qb] = jnp.concatenate([rows[:, 0], rows[:, 1]], axis=2).astype(BF16)
        for t in range(8):
            @pl.when(jnp.logical_not(is_me(qb, t)))
            def _():
                back(qb, t).start()

            @pl.when(is_me(qb, t))
            def _():
                att_all[4 * x + y] = o_rows[qb, t]

    @pl.loop(0, 11)
    def _(turn):
        s, b = turn // 2, lax.rem(turn, 2)
        for k in range(2):
            @pl.when(jnp.logical_and(b == k, turn < 10))
            def _():
                pass_on(s, k)

        @pl.when(turn == 1)
        def _():
            mix_pool()

        @pl.when(jnp.logical_and(turn == 1, 2 * c != y))
        def _():
            remote(q_own.at[0], q_in.at[0], q_send.at[0], q_recv.at[0], sib).wait_recv()

        @pl.when(turn == 1)
        def _():
            remote(q_own.at[0], q_in.at[1], q_send.at[0], q_recv.at[1], sib).wait_recv()

        @pl.when(turn == 4)
        def _():
            weights_out.relay_first()

        @pl.when(turn == 6)
        def _():
            weights_out.relay_second()

        @pl.when(turn == 8)
        def _():
            weights_out.relay_far()

        done = s - 1
        zb = lax.rem(z + 8 + jnp.where(b == 0, -done, done), 8)

        @pl.when(jnp.logical_and(turn >= 2, turn != 3))
        def _():
            unpack(zb)

            @pl.loop(0, 2)
            def _(i):
                use(zb, 1 - i)

                @pl.when(turn == 10)
                def _():
                    send_back(1 - i)

    for k in range(1, 8):
        idx = lax.rem(tp + k, 8)
        remote(pool_in.at[0], pool_in.at[idx], p_send.at[k], p_recv.at[idx], sib).wait_recv()
    for offset in (0, -1, 1, 2):
        weights_out.wait_sibling(offset)
    for t in range(8):
        lhs[:, pl.ds(t * 128, 128)] = pool_in[t]

    def out_part(first, part_of):
        columns = pl.ds(part_of * 512, 512)
        return dot(lhs[...], w_all[:, pl.ds(first, 128), columns].reshape(D // 2, 512)), columns

    for part_of in range(4):
        value, columns = out_part(0, part_of)
        total[:, columns] = value

    mine = jnp.logical_and(even, 2 * c == y)

    @pl.loop(0, 16)
    def _(head):
        @pl.when(jnp.logical_not(jnp.logical_and(mine, head == 4 * x + y)))
        def _():
            remote(att_all.at[0], att_all.at[head], o_send.at[0, 0], o_recv.at[head], sib).wait_recv()

    for t in range(8):
        two = [att_all[2 * t], att_all[2 * t + 1]]
        for h in range(2):
            rows = [value[:, h * 64 : h * 64 + 64] for value in two]
            lhs[pl.ds(h * HALF, HALF), pl.ds(t * 128, 128)] = jnp.concatenate(rows, axis=1)
    for part_of in range(4):
        value, columns = out_part(128, part_of)
        out_ref[:, columns] = (total[:, columns] + value).astype(BF16)

    acts.finish()
    kv_lats.finish()
    q_lats.finish()
    halo.wait_send()
    for j in range(2):
        @pl.when(jnp.logical_not(jnp.logical_and(even, 2 * c + j == y)))
        def _():
            q_copy(j).wait_send()

        @pl.when(2 * c + j != y)
        def _():
            kv_copy(j).wait_send()

    for qb in range(2):
        for t in range(8):
            @pl.when(jnp.logical_not(is_me(qb, t)))
            def _():
                back(qb, t).wait_send()

    for k in range(1, 8):
        pool_copy(k).wait_send()
    weights_out.finish()
    for b in range(2):
        for way in range(2):
            for s in range(4 if way == b else 3):
                ring_copy(0, way, b, s).wait_send()

    @pl.loop(0, 8)
    def _(zb):
        for b in range(2):
            sib_copy(zb * 4 + 2 * c + b).wait_send()


DMA = pltpu.SemaphoreType.DMA


def params(number):
    return pltpu.CompilerParams(collective_id=number, has_side_effects=True, vmem_limit_bytes=60 * 1024 * 1024)


def local(
    activations, in_gain, w_pool_in, pool_gain, w_qlat, w_kvlat, w_krope, qlat_gain, kvlat_gain,
    w_qup, w_kup, w_vup, qhead_gain, khead_gain, w_out_pool, w_out_attn,
):
    tables = [jnp.asarray(t) for t in rotary_tables()]
    gather_sems = [DMA((6,)), DMA((8,)), DMA((8, 2))]
    return pl.pallas_call(
        mixer_kernel,
        name="mixer",
        out_shape=jax.ShapeDtypeStruct((BLOCK, D), BF16),
        in_specs=[VMEM_SPEC] * 20,
        out_specs=VMEM_SPEC,
        scratch_shapes=[
            pltpu.VMEM((8, BLOCK, D), BF16),
            pltpu.VMEM((ROWS, 192), F32),
            pltpu.VMEM((64, ROWS), BF16),
            pltpu.VMEM((8, 64, ROWS), BF16),
            pltpu.VMEM((96, ROWS), BF16),
            pltpu.VMEM((8, 96, ROWS), BF16),
            pltpu.VMEM((HALO + ROWS, 128), F32),
            pltpu.VMEM((HALO, 128), BF16),
            pltpu.VMEM((HALO, 128), BF16),
            pltpu.VMEM((D, 192), BF16),
            pltpu.VMEM((256, KVLAT), BF16),
            pltpu.VMEM((2, HEAD, ROWS), BF16),
            pltpu.VMEM((2, LAT, ROWS), BF16),
            pltpu.VMEM((ROWS, 128), BF16),
            pltpu.VMEM((32, LAT, ROWS), BF16),
            pltpu.VMEM((32, ROWS, HEAD), BF16),
            pltpu.VMEM((2, HEAD, ROWS), BF16),
            pltpu.VMEM((2, VDIM, ROWS), F32),
            pltpu.VMEM((2, 8, ROWS), F32),
            pltpu.VMEM((2, 8, HALF, 128), BF16),
            pltpu.VMEM((16, HALF, 128), BF16),
            pltpu.VMEM((8, BLOCK, 128), BF16),
            pltpu.VMEM((8, 256, D), BF16),
            pltpu.VMEM((BLOCK, D // 2), BF16),
            pltpu.VMEM((BLOCK, D), F32),
            *gather_sems, *gather_sems, *gather_sems, DMA((2,)),
            DMA((2,)), DMA((32,)), DMA((2,)), DMA((2,)), DMA((2, 2, 4)), DMA((32,)), DMA((2, 8)), DMA((16,)),
            DMA((8,)), DMA((8,)), *gather_sems,
        ],
        compiler_params=params(1),
    )(
        activations, in_gain[None, :], w_pool_in, w_qlat.T, w_kvlat.T, w_krope.T, pool_gain[None, :], qlat_gain[None, :],
        kvlat_gain[None, :], w_qup.T, w_kup, w_vup, qhead_gain[None, :], khead_gain[None, :], *tables, w_out_pool, w_out_attn,
    )


def solution(mesh):
    placed = (
        P(("sp", "tp"), None), P(), P(None, "tp"), P("tp"), P(None, "tp"), P(None, "tp"), P(), P(), P(),
        P(None, "tp"), P(None, "tp"), P(None, "tp"), P(), P(), P("tp", None), P("tp", None),
    )
    return jax.shard_map(local, mesh=mesh, in_specs=placed, out_specs=P(("sp", "tp"), None), check_vma=False)
```

```python
import functools
import math

import jax
import jax.numpy as jnp
import numpy as np
from jax import lax
from jax.experimental import pallas as pl
from jax.experimental.pallas import tpu as pltpu
from jax.sharding import PartitionSpec as P

NOPE = 64
ROPE = 32
HEAD = NOPE + ROPE
VDIM = 64
QLAT = 768
KVLAT = 512
EPS = 1e-06
THETA = 10000.0
ROWS = 768
BLOCK = 96
HALF = BLOCK // 2
D = 2048
LAT = 160
HALO = 16
F32 = jnp.float32
BF16 = jnp.bfloat16
MESH = pl.DeviceIdType.MESH
VMEM_SPEC = pl.BlockSpec(memory_space=pltpu.VMEM)
SCALE = (1.0 / math.sqrt(HEAD)) * math.log2(math.e)


def dot(a, b):
    return jnp.dot(a, b, preferred_element_type=F32)


def turned(a):
    return jnp.transpose(a.astype(F32))


def column(row_ref):
    return jnp.transpose(jnp.broadcast_to(row_ref[...], (8, row_ref.shape[1])))[:, 0:1]


def rotary_tables():
    freq = THETA ** (-np.arange(0, ROPE, 2, dtype=np.float64) / ROPE)
    far = freq[:, None] * (np.arange(128, dtype=np.float64)[None, :] * ROWS)
    near = freq[:, None] * np.arange(ROWS, dtype=np.float64)[None, :]
    return tuple(t.astype(np.float32) for t in (np.cos(far), np.sin(far), np.cos(near), np.sin(near)))


def place():
    sp = lax.axis_index("sp")
    tp = lax.axis_index("tp")
    return sp, tp, tp // 2, lax.rem(tp, 2)


def meet(devices):
    barrier = pltpu.get_barrier_semaphore()
    for device in devices:
        pl.semaphore_signal(barrier, inc=1, device_id=device, device_id_type=MESH)
    pl.semaphore_wait(barrier, len(devices))


def remote(src, dst, send_sem, recv_sem, device):
    return pltpu.make_async_remote_copy(
        src_ref=src, dst_ref=dst, send_sem=send_sem, recv_sem=recv_sem, device_id=device, device_id_type=MESH
    )


class TpGather:
    def __init__(self, own, everything, half, sp, x, c, ring_send, sib_send, recv):
        self.own, self.all, self.half = own, everything, half
        self.x, self.c = x, c
        self.ring_send, self.sib_send, self.recv = ring_send, sib_send, recv
        self.right = {"sp": sp, "tp": lax.rem(x + 1, 4) * 2 + c}
        self.left = {"sp": sp, "tp": lax.rem(x + 3, 4) * 2 + c}
        self.sib = {"sp": sp, "tp": x * 2 + 1 - c}

    def index(self, offset, core):
        return lax.rem(self.x + 4 + offset, 4) * 2 + core

    def piece(self, idx, h):
        return self.all.at[idx, pl.ds(h * self.half, self.half)]

    def copy(self, src, idx, h, send, device):
        return remote(src, self.piece(idx, h), send, self.recv.at[idx, h], device)

    def start(self):
        me = self.index(0, self.c)
        for k, (device, h) in enumerate(((self.right, 0), (self.left, 1), (self.right, 1), (self.left, 0))):
            self.copy(self.own[h], me, h, self.ring_send.at[k], device).start()
        for h in range(2):
            self.copy(self.own[h], me, h, self.sib_send.at[h], self.sib).start()

    def wait_piece(self, idx, h):
        self.copy(self.own[h], idx, h, self.sib_send.at[0], self.sib).wait_recv()

    def got(self, offset, h, slot, onward=None, onward_slot=0):
        idx = self.index(offset, self.c)
        self.wait_piece(idx, h)
        if onward is not None:
            self.copy(self.piece(idx, h), idx, h, self.ring_send.at[onward_slot], onward).start()
        self.copy(self.piece(idx, h), idx, h, self.sib_send.at[slot], self.sib).start()

    def relay_first(self):
        self.got(-1, 0, 2, self.right, 4)
        self.got(1, 1, 3, self.left, 5)

    def relay_second(self):
        self.got(-1, 1, 4)
        self.got(1, 0, 5)

    def relay_far(self):
        self.got(2, 0, 6)
        self.got(2, 1, 7)

    def wait_sibling(self, offset):
        idx = self.index(offset, 1 - self.c)
        for h in range(2):
            self.wait_piece(idx, h)
        return idx

    def finish(self):
        for k in range(6):
            self.copy(self.own[0], 0, 0, self.ring_send.at[k], self.sib).wait_send()
        for k in range(8):
            self.copy(self.own[0], 0, 0, self.sib_send.at[k], self.sib).wait_send()


def mixer_kernel(
    act, in_gain, w_pool, w_qlat_t, w_kvlat_t, w_krope_t, pool_gain, q_gain, kv_gain, wq_t, w_kup, w_vup, qh_gain, kh_gain,
    far_cos, far_sin, near_cos, near_sin, w_out_pool, w_out_attn,
    out_ref,
    act_all, lat_rows, kvl_own, kvl_all, ql_own, ql_all, pool_rows, halo_out, halo_in, w_lat, wkv_t, q_own, kv_own, pool_own,
    kv_all, k_rows, q_in, acc, den, o_rows, att_all, pool_in, w_all, lhs, total,
    a_ring, a_sib, a_recv, k_ring, k_sib, k_recv, l_ring, l_sib, l_recv, halo_sem,
    c_send, kv_recv, q_send, q_recv, ring_send, sib_send, o_send, o_recv, p_send, p_recv, w_ring, w_sib, w_recv,
):
    sp, tp, x, c = place()
    z, y = sp // 4, lax.rem(sp, 4)
    even = lax.rem(y, 2) == 0
    owner = y // 2
    q_c = jnp.where(y < 2, y, 3 - y)

    def device(yy, zz, cc, xx=x):
        return {"sp": zz * 4 + yy, "tp": xx * 2 + cc}

    up = device(y, lax.rem(z + 1, 8), c)
    down = device(y, lax.rem(z + 7, 8), c)
    sib = device(y, z, 1 - c)
    behind = {"sp": lax.rem(sp + 1, 32), "tp": tp}
    before = {"sp": lax.rem(sp + 31, 32), "tp": tp}

    def gather(own, everything, half, *sems):
        return TpGather(own, everything, half, sp, x, c, *sems)

    acts = gather([act.at[pl.ds(0, HALF)], act.at[pl.ds(HALF, HALF)]], act_all, HALF, a_ring, a_sib, a_recv)
    kv_lats = gather([kvl_own.at[pl.ds(0, 32)], kvl_own.at[pl.ds(32, 32)]], kvl_all, 32, k_ring, k_sib, k_recv)
    q_lats = gather([ql_own.at[pl.ds(0, 48)], ql_own.at[pl.ds(48, 48)]], ql_all, 48, l_ring, l_sib, l_recv)
    weights_out = gather([w_out_pool, w_out_attn], w_all, 128, w_ring, w_sib, w_recv)

    friends = [up, down, behind, before]
    for dy in range(4):
        for dc in range(2):
            yy, cc = lax.rem(y + dy, 4), lax.rem(c + dc, 2)
            if dy or dc:
                friends.append(device(yy, z, cc))
    friends += [{"sp": sp, "tp": lax.rem(tp + k, 8)} for k in range(1, 8)]
    for dx in range(1, 4):
        for dy in range(4):
            friends.append(device(lax.rem(y + dy, 4), z, q_c, lax.rem(x + dx, 4)))
    meet(friends)

    acts.start()

    def project(block, idx):
        rows = pl.multiple_of(idx * BLOCK, 32)
        value = block[...].astype(F32)
        factor = lax.rsqrt(jnp.mean(value * value, axis=1, keepdims=True) + EPS)
        normed = (value * factor * in_gain[...]).astype(BF16)
        pool_rows[pl.ds(HALO + rows, BLOCK), :] = dot(normed, w_pool[...]).astype(BF16).astype(F32)
        lat_rows[pl.ds(rows, BLOCK), :] = dot(normed, w_lat[...])

    w_lat[...] = turned(jnp.concatenate([w_qlat_t[...], w_kvlat_t[...], w_krope_t[...]], axis=0)).astype(BF16)
    project(act, tp)
    wkv_t[pl.ds(0, 128), :] = turned(w_kup[...]).astype(BF16)
    wkv_t[pl.ds(128, 128), :] = turned(w_vup[...]).astype(BF16)
    idx = acts.wait_sibling(0)
    project(act_all.at[idx], idx)
    acts.relay_first()
    acts.relay_second()
    for offset in (-1, 1):
        idx = acts.index(offset, c)
        project(act_all.at[idx], idx)
    for offset in (-1, 1):
        idx = acts.wait_sibling(offset)
        project(act_all.at[idx], idx)
    acts.relay_far()
    idx = acts.index(2, c)
    project(act_all.at[idx], idx)
    idx = acts.wait_sibling(2)
    project(act_all.at[idx], idx)

    lat_t = jnp.transpose(lat_rows[...])
    kvl_own[...] = lat_t[96:160].astype(BF16)
    ql_own[...] = lat_t[0:96].astype(BF16)
    rope_t = lat_t[160:192].astype(BF16).astype(F32)
    halo_out[...] = pool_rows[pl.ds(ROWS, HALO), :].astype(BF16)
    kv_lats.start()
    halo = remote(halo_out, halo_in, halo_sem.at[0], halo_sem.at[1], behind)
    halo.start()
    kvl_all[tp] = kvl_own[...]
    ql_all[tp] = ql_own[...]

    column_of = lax.broadcasted_iota(jnp.int32, (16, 128), 1) == sp
    cos = jnp.sum(jnp.where(column_of, far_cos[...], 0.0), axis=1, keepdims=True)
    sin = jnp.sum(jnp.where(column_of, far_sin[...], 0.0), axis=1, keepdims=True)
    cosine = cos * near_cos[...] - sin * near_sin[...]
    sine = sin * near_cos[...] + cos * near_sin[...]

    kv_lats.relay_first()
    q_lats.start()
    kv_lats.relay_second()
    kv_lats.relay_far()
    for offset in (0, -1, 1, 2):
        kv_lats.wait_sibling(offset)

    def finish(head, gain):
        factor = lax.rsqrt(jnp.sum(head * head, axis=0, keepdims=True) / HEAD + EPS)
        head = head * factor * gain
        lower, upper = head[64:80], head[80:96]
        return jnp.concatenate([head[:64], lower * cosine - upper * sine, upper * cosine + lower * sine], axis=0)

    kv_lat = kvl_all[...].reshape(KVLAT, ROWS).astype(F32)
    kv_norm = kv_lat * lax.rsqrt(jnp.sum(kv_lat * kv_lat, axis=0, keepdims=True) / KVLAT + EPS) * column(kv_gain)
    plain = dot(wkv_t[...], kv_norm.astype(BF16)).astype(BF16)
    for h in range(2):
        joined = jnp.concatenate([plain[h * 64 : h * 64 + 64].astype(F32), rope_t], axis=0)
        kv_own[h, 0:96, :] = finish(joined, column(kh_gain)).astype(BF16)
        kv_own[h, 96:160, :] = plain[128 + h * 64 : 192 + h * 64]

    def kv_copy(j):
        return remote(kv_own.at[j], kv_all.at[sp], c_send.at[j], kv_recv.at[sp], device(2 * c + j, z, owner))

    def q_copy(j):
        return remote(q_own.at[j], q_in.at[owner], q_send.at[j], q_recv.at[owner], device(2 * c + j, z, q_c))

    for j in range(2):
        here = 2 * c + j == y

        @pl.when(jnp.logical_not(here))
        def _():
            kv_copy(j).start()

        @pl.when(here)
        def _():
            kv_all[sp] = kv_own[j]

    q_lats.relay_first()
    q_lats.relay_second()
    q_lats.relay_far()
    for offset in (0, -1, 1, 2):
        q_lats.wait_sibling(offset)
    weights_out.start()
    q_lat = ql_all[...].reshape(QLAT, ROWS).astype(F32)
    q_norm = q_lat * lax.rsqrt(jnp.sum(q_lat * q_lat, axis=0, keepdims=True) / QLAT + EPS) * column(q_gain)
    raw = dot(wq_t[...], q_norm.astype(BF16)).astype(BF16).astype(F32)
    for h in range(2):
        q_own[h] = (finish(raw[h * 96 : h * 96 + 96], column(qh_gain)) * SCALE).astype(BF16)

    for j in range(2):
        here = jnp.logical_and(even, 2 * c + j == y)

        @pl.when(jnp.logical_not(here))
        def _():
            q_copy(j).start()

        @pl.when(here)
        def _():
            q_in[owner] = q_own[j]

    def wait_slot(slot):
        remote(kv_all.at[slot], kv_all.at[slot], sib_send.at[slot], kv_recv.at[slot], sib).wait_recv()

    def ring_copy(slot, way, b, s):
        return remote(kv_all.at[slot], kv_all.at[slot], ring_send.at[way, b, s], kv_recv.at[slot], (up, down)[way])

    def sib_copy(slot):
        return remote(kv_all.at[slot], kv_all.at[slot], sib_send.at[slot], kv_recv.at[slot], sib)

    def pool_copy(k):
        to = lax.rem(tp + k, 8)
        rows = pl.multiple_of(to * BLOCK, 32)
        return remote(pool_own.at[pl.ds(rows, BLOCK)], pool_in.at[tp], p_send.at[k], p_recv.at[tp], {"sp": sp, "tp": to})

    def mix_pool():
        halo.wait_recv()
        pool_rows[pl.ds(0, HALO), :] = jnp.where(sp > 0, halo_in[...].astype(F32), 0.0)
        window = jnp.left_shift(jnp.int32(2), tp // 2)
        summed = jnp.zeros((ROWS, 128), F32)
        for lag in range(16):
            summed = summed + jnp.where(lag < window, pool_rows[pl.ds(HALO - lag, ROWS), :], 0.0)
        position = sp * ROWS + lax.broadcasted_iota(jnp.int32, (ROWS, 128), 0)
        divisor = jnp.minimum(position + 1, window).astype(F32)
        pooled = summed / divisor - pool_rows[pl.ds(HALO, ROWS), :]
        pool_own[...] = (pooled * pool_gain[...]).astype(BF16)
        for k in range(1, 8):
            pool_copy(k).start()
        pool_in[tp] = pool_own[pl.ds(pl.multiple_of(tp * BLOCK, 32), BLOCK), :]
        w_all[tp, pl.ds(0, 128), :] = w_out_pool[...]
        w_all[tp, pl.ds(128, 128), :] = w_out_attn[...]
        acc[...] = jnp.zeros_like(acc)
        den[...] = jnp.zeros_like(den)

    def attend(slots, qb, diagonal):
        units = [(slot, qc) for slot in slots for qc in range(3)]

        def score(unit):
            slot, qc = unit
            keys = (qc + 1) * 256 if diagonal else ROWS
            return dot(k_rows[slot, pl.ds(0, keys), :], q_in[qb, :, pl.ds(qc * 256, 256)])

        ready = [score(unit) for unit in units[:2]]
        for i, (slot, qc) in enumerate(units):
            if i + 2 < len(units):
                ready.append(score(units[i + 2]))
            columns = pl.ds(qc * 256, 256)
            keys = (qc + 1) * 256 if diagonal else ROWS
            weights = jnp.exp2(ready.pop(0))
            if diagonal:
                k_pos = lax.broadcasted_iota(jnp.int32, (keys, 256), 0)
                q_pos = lax.broadcasted_iota(jnp.int32, (keys, 256), 1) + qc * 256
                weights = jnp.where(k_pos <= q_pos, weights, 0.0)
            den[qb, :, columns] += jnp.sum(weights.reshape(keys // 8, 8, 256), axis=0)
            acc[qb, :, columns] += dot(kv_all[slot, pl.ds(96, 64), pl.ds(0, keys)], weights.astype(BF16))

    def plane_of(way, s):
        return lax.rem(z + 8 - s, 8) if way == 0 else lax.rem(z + s, 8)

    def pass_on(s, b):
        @pl.when(jnp.logical_and(s == 0, 2 * c + b != y))
        def _():
            wait_slot(z * 4 + 2 * c + b)

        for way in ((0, 1), (1, 0))[b]:
            limit = 4 if way == b else 3
            slot = plane_of(way, s) * 4 + 2 * c + b

            @pl.when(jnp.logical_and(s >= 1, s <= limit))
            def _():
                wait_slot(slot)

            @pl.when(s < limit)
            def _():
                ring_copy(slot, way, b, s).start()

            @pl.when(jnp.logical_and(jnp.logical_or(s >= 1, way == 0), s <= limit))
            def _():
                sib_copy(slot).start()

    def query_row(qb):
        return jnp.where(qb == 0, c, 3 - c)

    def unpack(zb):
        first = zb * 4
        for b in range(2):
            wait_slot(first + 2 * (1 - c) + b)

        @pl.when(zb <= z)
        def _():
            for yb in range(4):
                k_rows[first + yb] = turned(kv_all[first + yb, pl.ds(0, HEAD), :]).astype(BF16)

    def use(zb, qb):
        first = zb * 4
        row = query_row(qb)

        @pl.when(zb < z)
        def _():
            attend([first + yb for yb in range(4)], qb, False)

        @pl.when(zb == z)
        def _():
            @pl.loop(0, row)
            def _(yb):
                attend([first + yb], qb, False)

            attend([first + row], qb, True)

    def back(qb, t):
        return remote(
            o_rows.at[qb, t], att_all.at[4 * x + y], o_send.at[qb, t], o_recv.at[4 * x + y],
            {"sp": z * 4 + query_row(qb), "tp": t},
        )

    def is_me(qb, t):
        return jnp.logical_and(query_row(qb) == y, tp == t)

    def send_back(qb):
        rows = jnp.transpose(acc[qb] / jnp.sum(den[qb], axis=0, keepdims=True)).reshape(8, 2, HALF, VDIM)
        o_rows[qb] = jnp.concatenate([rows[:, 0], rows[:, 1]], axis=2).astype(BF16)
        for t in range(8):
            @pl.when(jnp.logical_not(is_me(qb, t)))
            def _():
                back(qb, t).start()

            @pl.when(is_me(qb, t))
            def _():
                att_all[4 * x + y] = o_rows[qb, t]

    @pl.loop(0, 11)
    def _(turn):
        s, b = turn // 2, lax.rem(turn, 2)
        for k in range(2):
            @pl.when(jnp.logical_and(b == k, turn < 10))
            def _():
                pass_on(s, k)

        @pl.when(turn == 1)
        def _():
            mix_pool()

        for qb in range(2):
            kept = jnp.logical_and(jnp.logical_and(even, 2 * c == y), owner == qb)

            @pl.when(jnp.logical_and(turn == 1, jnp.logical_not(kept)))
            def _():
                remote(q_own.at[0], q_in.at[qb], q_send.at[0], q_recv.at[qb], sib).wait_recv()

        @pl.when(turn == 4)
        def _():
            weights_out.relay_first()

        @pl.when(turn == 6)
        def _():
            weights_out.relay_second()

        @pl.when(turn == 8)
        def _():
            weights_out.relay_far()

        done = s - 1
        zb = lax.rem(z + 8 + jnp.where(b == 0, -done, done), 8)

        @pl.when(jnp.logical_and(turn >= 2, turn != 3))
        def _():
            unpack(zb)

            @pl.loop(0, 2)
            def _(i):
                use(zb, 1 - i)

                @pl.when(turn == 10)
                def _():
                    send_back(1 - i)

    for k in range(1, 8):
        idx = lax.rem(tp + k, 8)
        remote(pool_in.at[0], pool_in.at[idx], p_send.at[k], p_recv.at[idx], sib).wait_recv()
    for offset in (0, -1, 1, 2):
        weights_out.wait_sibling(offset)
    for t in range(8):
        lhs[:, pl.ds(t * 128, 128)] = pool_in[t]

    def out_part(first, part_of):
        columns = pl.ds(part_of * 512, 512)
        return dot(lhs[...], w_all[:, pl.ds(first, 128), columns].reshape(D // 2, 512)), columns

    for part_of in range(4):
        value, columns = out_part(0, part_of)
        total[:, columns] = value

    mine = q_c == c

    @pl.loop(0, 16)
    def _(head):
        @pl.when(jnp.logical_not(jnp.logical_and(mine, head == 4 * x + y)))
        def _():
            remote(att_all.at[0], att_all.at[head], o_send.at[0, 0], o_recv.at[head], sib).wait_recv()

    for t in range(8):
        two = [att_all[2 * t], att_all[2 * t + 1]]
        for h in range(2):
            rows = [value[:, h * 64 : h * 64 + 64] for value in two]
            lhs[pl.ds(h * HALF, HALF), pl.ds(t * 128, 128)] = jnp.concatenate(rows, axis=1)
    for part_of in range(4):
        value, columns = out_part(128, part_of)
        out_ref[:, columns] = (total[:, columns] + value).astype(BF16)

    acts.finish()
    kv_lats.finish()
    q_lats.finish()
    halo.wait_send()
    for j in range(2):
        @pl.when(jnp.logical_not(jnp.logical_and(even, 2 * c + j == y)))
        def _():
            q_copy(j).wait_send()

        @pl.when(2 * c + j != y)
        def _():
            kv_copy(j).wait_send()

    for qb in range(2):
        for t in range(8):
            @pl.when(jnp.logical_not(is_me(qb, t)))
            def _():
                back(qb, t).wait_send()

    for k in range(1, 8):
        pool_copy(k).wait_send()
    weights_out.finish()
    for b in range(2):
        for way in range(2):
            for s in range(4 if way == b else 3):
                ring_copy(0, way, b, s).wait_send()

    @pl.loop(0, 8)
    def _(zb):
        for b in range(2):
            sib_copy(zb * 4 + 2 * c + b).wait_send()


DMA = pltpu.SemaphoreType.DMA


def params(number):
    return pltpu.CompilerParams(collective_id=number, has_side_effects=True, vmem_limit_bytes=60 * 1024 * 1024)


def local(
    activations, in_gain, w_pool_in, pool_gain, w_qlat, w_kvlat, w_krope, qlat_gain, kvlat_gain,
    w_qup, w_kup, w_vup, qhead_gain, khead_gain, w_out_pool, w_out_attn,
):
    tables = [jnp.asarray(t) for t in rotary_tables()]
    gather_sems = [DMA((6,)), DMA((8,)), DMA((8, 2))]
    return pl.pallas_call(
        mixer_kernel,
        name="mixer",
        out_shape=jax.ShapeDtypeStruct((BLOCK, D), BF16),
        in_specs=[VMEM_SPEC] * 20,
        out_specs=VMEM_SPEC,
        scratch_shapes=[
            pltpu.VMEM((8, BLOCK, D), BF16),
            pltpu.VMEM((ROWS, 192), F32),
            pltpu.VMEM((64, ROWS), BF16),
            pltpu.VMEM((8, 64, ROWS), BF16),
            pltpu.VMEM((96, ROWS), BF16),
            pltpu.VMEM((8, 96, ROWS), BF16),
            pltpu.VMEM((HALO + ROWS, 128), F32),
            pltpu.VMEM((HALO, 128), BF16),
            pltpu.VMEM((HALO, 128), BF16),
            pltpu.VMEM((D, 192), BF16),
            pltpu.VMEM((256, KVLAT), BF16),
            pltpu.VMEM((2, HEAD, ROWS), BF16),
            pltpu.VMEM((2, LAT, ROWS), BF16),
            pltpu.VMEM((ROWS, 128), BF16),
            pltpu.VMEM((32, LAT, ROWS), BF16),
            pltpu.VMEM((32, ROWS, HEAD), BF16),
            pltpu.VMEM((2, HEAD, ROWS), BF16),
            pltpu.VMEM((2, VDIM, ROWS), F32),
            pltpu.VMEM((2, 8, ROWS), F32),
            pltpu.VMEM((2, 8, HALF, 128), BF16),
            pltpu.VMEM((16, HALF, 128), BF16),
            pltpu.VMEM((8, BLOCK, 128), BF16),
            pltpu.VMEM((8, 256, D), BF16),
            pltpu.VMEM((BLOCK, D // 2), BF16),
            pltpu.VMEM((BLOCK, D), F32),
            *gather_sems, *gather_sems, *gather_sems, DMA((2,)),
            DMA((2,)), DMA((32,)), DMA((2,)), DMA((2,)), DMA((2, 2, 4)), DMA((32,)), DMA((2, 8)), DMA((16,)),
            DMA((8,)), DMA((8,)), *gather_sems,
        ],
        compiler_params=params(1),
    )(
        activations, in_gain[None, :], w_pool_in, w_qlat.T, w_kvlat.T, w_krope.T, pool_gain[None, :], qlat_gain[None, :],
        kvlat_gain[None, :], w_qup.T, w_kup, w_vup, qhead_gain[None, :], khead_gain[None, :], *tables, w_out_pool, w_out_attn,
    )


def solution(mesh):
    placed = (
        P(("sp", "tp"), None), P(), P(None, "tp"), P("tp"), P(None, "tp"), P(None, "tp"), P(), P(), P(),
        P(None, "tp"), P(None, "tp"), P(None, "tp"), P(), P(), P("tp", None), P("tp", None),
    )
    return jax.shard_map(local, mesh=mesh, in_specs=placed, out_specs=P(("sp", "tp"), None), check_vma=False)
```

```python
import functools
import math

import jax
import jax.numpy as jnp
import numpy as np
from jax import lax
from jax.experimental import pallas as pl
from jax.experimental.pallas import tpu as pltpu
from jax.sharding import PartitionSpec as P

NOPE = 64
ROPE = 32
HEAD = NOPE + ROPE
VDIM = 64
QLAT = 768
KVLAT = 512
EPS = 1e-06
THETA = 10000.0
ROWS = 768
BLOCK = 96
HALF = BLOCK // 2
D = 2048
LAT = 160
HALO = 16
F32 = jnp.float32
BF16 = jnp.bfloat16
MESH = pl.DeviceIdType.MESH
VMEM_SPEC = pl.BlockSpec(memory_space=pltpu.VMEM)
SCALE = (1.0 / math.sqrt(HEAD)) * math.log2(math.e)


def dot(a, b):
    return jnp.dot(a, b, preferred_element_type=F32)


def turned(a):
    return jnp.transpose(a.astype(F32))


def column(row_ref):
    return jnp.transpose(jnp.broadcast_to(row_ref[...], (8, row_ref.shape[1])))[:, 0:1]


def rotary_tables():
    freq = THETA ** (-np.arange(0, ROPE, 2, dtype=np.float64) / ROPE)
    far = freq[:, None] * (np.arange(128, dtype=np.float64)[None, :] * ROWS)
    near = freq[:, None] * np.arange(ROWS, dtype=np.float64)[None, :]
    return tuple(t.astype(np.float32) for t in (np.cos(far), np.sin(far), np.cos(near), np.sin(near)))


def place():
    sp = lax.axis_index("sp")
    tp = lax.axis_index("tp")
    return sp, tp, tp // 2, lax.rem(tp, 2)


def meet(devices):
    barrier = pltpu.get_barrier_semaphore()
    for device in devices:
        pl.semaphore_signal(barrier, inc=1, device_id=device, device_id_type=MESH)
    pl.semaphore_wait(barrier, len(devices))


def remote(src, dst, send_sem, recv_sem, device):
    return pltpu.make_async_remote_copy(
        src_ref=src, dst_ref=dst, send_sem=send_sem, recv_sem=recv_sem, device_id=device, device_id_type=MESH
    )


class TpGather:
    def __init__(self, own, everything, half, sp, x, c, ring_send, sib_send, recv):
        self.own, self.all, self.half = own, everything, half
        self.x, self.c = x, c
        self.ring_send, self.sib_send, self.recv = ring_send, sib_send, recv
        self.right = {"sp": sp, "tp": lax.rem(x + 1, 4) * 2 + c}
        self.left = {"sp": sp, "tp": lax.rem(x + 3, 4) * 2 + c}
        self.sib = {"sp": sp, "tp": x * 2 + 1 - c}

    def index(self, offset, core):
        return lax.rem(self.x + 4 + offset, 4) * 2 + core

    def piece(self, idx, h):
        return self.all.at[idx, pl.ds(h * self.half, self.half)]

    def copy(self, src, idx, h, send, device):
        return remote(src, self.piece(idx, h), send, self.recv.at[idx, h], device)

    def start(self):
        me = self.index(0, self.c)
        for k, (device, h) in enumerate(((self.right, 0), (self.left, 1), (self.right, 1), (self.left, 0))):
            self.copy(self.own[h], me, h, self.ring_send.at[k], device).start()
        for h in range(2):
            self.copy(self.own[h], me, h, self.sib_send.at[h], self.sib).start()

    def wait_piece(self, idx, h):
        self.copy(self.own[h], idx, h, self.sib_send.at[0], self.sib).wait_recv()

    def got(self, offset, h, slot, onward=None, onward_slot=0):
        idx = self.index(offset, self.c)
        self.wait_piece(idx, h)
        if onward is not None:
            self.copy(self.piece(idx, h), idx, h, self.ring_send.at[onward_slot], onward).start()
        self.copy(self.piece(idx, h), idx, h, self.sib_send.at[slot], self.sib).start()

    def relay_first(self):
        self.got(-1, 0, 2, self.right, 4)
        self.got(1, 1, 3, self.left, 5)

    def relay_second(self):
        self.got(-1, 1, 4)
        self.got(1, 0, 5)

    def relay_far(self):
        self.got(2, 0, 6)
        self.got(2, 1, 7)

    def wait_sibling(self, offset):
        idx = self.index(offset, 1 - self.c)
        for h in range(2):
            self.wait_piece(idx, h)
        return idx

    def finish(self):
        for k in range(6):
            self.copy(self.own[0], 0, 0, self.ring_send.at[k], self.sib).wait_send()
        for k in range(8):
            self.copy(self.own[0], 0, 0, self.sib_send.at[k], self.sib).wait_send()


def mixer_kernel(
    act, in_gain, w_pool, w_qlat_t, w_kvlat_t, w_krope_t, pool_gain, q_gain, kv_gain, wq_t, w_kup, w_vup, qh_gain, kh_gain,
    far_cos, far_sin, near_cos, near_sin, w_out_pool, w_out_attn,
    out_ref,
    act_all, lat_rows, kvl_own, kvl_all, ql_own, ql_all, pool_rows, halo_out, halo_in, w_lat, wkv_t, q_own, kv_own, pool_own,
    kv_all, k_rows, q_in, acc, den, o_rows, att_all, pool_in, w_all, lhs, total,
    a_ring, a_sib, a_recv, k_ring, k_sib, k_recv, l_ring, l_sib, l_recv, halo_sem,
    c_send, kv_recv, q_send, q_recv, ring_send, sib_send, o_send, o_recv, p_send, p_recv, w_ring, w_sib, w_recv,
):
    sp, tp, x, c = place()
    z, y = sp // 4, lax.rem(sp, 4)
    even = lax.rem(y, 2) == 0
    owner = y // 2
    q_c = jnp.where(y < 2, y, 3 - y)

    def device(yy, zz, cc, xx=x):
        return {"sp": zz * 4 + yy, "tp": xx * 2 + cc}

    up = device(y, lax.rem(z + 1, 8), c)
    down = device(y, lax.rem(z + 7, 8), c)
    sib = device(y, z, 1 - c)
    behind = {"sp": lax.rem(sp + 1, 32), "tp": tp}
    before = {"sp": lax.rem(sp + 31, 32), "tp": tp}

    def gather(own, everything, half, *sems):
        return TpGather(own, everything, half, sp, x, c, *sems)

    acts = gather([act.at[pl.ds(0, HALF)], act.at[pl.ds(HALF, HALF)]], act_all, HALF, a_ring, a_sib, a_recv)
    kv_lats = gather([kvl_own.at[pl.ds(0, 32)], kvl_own.at[pl.ds(32, 32)]], kvl_all, 32, k_ring, k_sib, k_recv)
    q_lats = gather([ql_own.at[pl.ds(0, 48)], ql_own.at[pl.ds(48, 48)]], ql_all, 48, l_ring, l_sib, l_recv)
    weights_out = gather([w_out_pool, w_out_attn], w_all, 128, w_ring, w_sib, w_recv)

    friends = [up, down, behind, before]
    for dy in range(4):
        for dc in range(2):
            yy, cc = lax.rem(y + dy, 4), lax.rem(c + dc, 2)
            if dy or dc:
                friends.append(device(yy, z, cc))
    friends += [{"sp": sp, "tp": lax.rem(tp + k, 8)} for k in range(1, 8)]
    for dx in range(1, 4):
        for dy in range(4):
            friends.append(device(lax.rem(y + dy, 4), z, q_c, lax.rem(x + dx, 4)))
    meet(friends)

    acts.start()

    def project(block, idx):
        rows = pl.multiple_of(idx * BLOCK, 32)
        value = block[...].astype(F32)
        factor = lax.rsqrt(jnp.mean(value * value, axis=1, keepdims=True) + EPS)
        normed = (value * factor * in_gain[...]).astype(BF16)
        pool_rows[pl.ds(HALO + rows, BLOCK), :] = dot(normed, w_pool[...]).astype(BF16).astype(F32)
        lat_rows[pl.ds(rows, BLOCK), :] = dot(normed, w_lat[...])

    w_lat[...] = turned(jnp.concatenate([w_qlat_t[...], w_kvlat_t[...], w_krope_t[...]], axis=0)).astype(BF16)
    project(act, tp)
    wkv_t[pl.ds(0, 128), :] = turned(w_kup[...]).astype(BF16)
    wkv_t[pl.ds(128, 128), :] = turned(w_vup[...]).astype(BF16)
    idx = acts.wait_sibling(0)
    project(act_all.at[idx], idx)
    acts.relay_first()
    acts.relay_second()
    for offset in (-1, 1):
        idx = acts.index(offset, c)
        project(act_all.at[idx], idx)
    for offset in (-1, 1):
        idx = acts.wait_sibling(offset)
        project(act_all.at[idx], idx)
    acts.relay_far()
    idx = acts.index(2, c)
    project(act_all.at[idx], idx)
    idx = acts.wait_sibling(2)
    project(act_all.at[idx], idx)

    lat_t = jnp.transpose(lat_rows[...])
    kvl_own[...] = lat_t[96:160].astype(BF16)
    ql_own[...] = lat_t[0:96].astype(BF16)
    rope_t = lat_t[160:192].astype(BF16).astype(F32)
    halo_out[...] = pool_rows[pl.ds(ROWS, HALO), :].astype(BF16)
    kv_lats.start()
    halo = remote(halo_out, halo_in, halo_sem.at[0], halo_sem.at[1], behind)
    halo.start()
    kvl_all[tp] = kvl_own[...]
    ql_all[tp] = ql_own[...]

    column_of = lax.broadcasted_iota(jnp.int32, (16, 128), 1) == sp
    cos = jnp.sum(jnp.where(column_of, far_cos[...], 0.0), axis=1, keepdims=True)
    sin = jnp.sum(jnp.where(column_of, far_sin[...], 0.0), axis=1, keepdims=True)
    cosine = cos * near_cos[...] - sin * near_sin[...]
    sine = sin * near_cos[...] + cos * near_sin[...]

    kv_lats.relay_first()
    q_lats.start()
    kv_lats.relay_second()
    kv_lats.relay_far()
    for offset in (0, -1, 1, 2):
        kv_lats.wait_sibling(offset)

    def finish(head, gain):
        factor = lax.rsqrt(jnp.sum(head * head, axis=0, keepdims=True) / HEAD + EPS)
        head = head * factor * gain
        lower, upper = head[64:80], head[80:96]
        return jnp.concatenate([head[:64], lower * cosine - upper * sine, upper * cosine + lower * sine], axis=0)

    kv_lat = kvl_all[...].reshape(KVLAT, ROWS).astype(F32)
    kv_norm = kv_lat * lax.rsqrt(jnp.sum(kv_lat * kv_lat, axis=0, keepdims=True) / KVLAT + EPS) * column(kv_gain)
    plain = dot(wkv_t[...], kv_norm.astype(BF16)).astype(BF16)
    for h in range(2):
        joined = jnp.concatenate([plain[h * 64 : h * 64 + 64].astype(F32), rope_t], axis=0)
        kv_own[h, 0:96, :] = finish(joined, column(kh_gain)).astype(BF16)
        kv_own[h, 96:160, :] = plain[128 + h * 64 : 192 + h * 64]

    def kv_copy(j):
        return remote(kv_own.at[j], kv_all.at[sp], c_send.at[j], kv_recv.at[sp], device(2 * c + j, z, owner))

    def q_copy(j):
        return remote(q_own.at[j], q_in.at[owner], q_send.at[j], q_recv.at[owner], device(2 * c + j, z, q_c))

    for j in range(2):
        here = 2 * c + j == y

        @pl.when(jnp.logical_not(here))
        def _():
            kv_copy(j).start()

        @pl.when(here)
        def _():
            kv_all[sp] = kv_own[j]

    def pool_copy(k):
        to = lax.rem(tp + k, 8)
        rows = pl.multiple_of(to * BLOCK, 32)
        return remote(pool_own.at[pl.ds(rows, BLOCK)], pool_in.at[tp], p_send.at[k], p_recv.at[tp], {"sp": sp, "tp": to})

    def mix_pool():
        halo.wait_recv()
        pool_rows[pl.ds(0, HALO), :] = jnp.where(sp > 0, halo_in[...].astype(F32), 0.0)
        window = jnp.left_shift(jnp.int32(2), tp // 2)
        summed = jnp.zeros((ROWS, 128), F32)
        for lag in range(16):
            summed = summed + jnp.where(lag < window, pool_rows[pl.ds(HALO - lag, ROWS), :], 0.0)
        position = sp * ROWS + lax.broadcasted_iota(jnp.int32, (ROWS, 128), 0)
        divisor = jnp.minimum(position + 1, window).astype(F32)
        pooled = summed / divisor - pool_rows[pl.ds(HALO, ROWS), :]
        pool_own[...] = (pooled * pool_gain[...]).astype(BF16)
        for k in range(1, 8):
            pool_copy(k).start()
        pool_in[tp] = pool_own[pl.ds(pl.multiple_of(tp * BLOCK, 32), BLOCK), :]
        w_all[tp, pl.ds(0, 128), :] = w_out_pool[...]
        w_all[tp, pl.ds(128, 128), :] = w_out_attn[...]
        acc[...] = jnp.zeros_like(acc)
        den[...] = jnp.zeros_like(den)

    q_lats.relay_first()
    q_lats.relay_second()
    mix_pool()
    q_lats.relay_far()
    for offset in (0, -1, 1, 2):
        q_lats.wait_sibling(offset)
    weights_out.start()
    q_lat = ql_all[...].reshape(QLAT, ROWS).astype(F32)
    q_norm = q_lat * lax.rsqrt(jnp.sum(q_lat * q_lat, axis=0, keepdims=True) / QLAT + EPS) * column(q_gain)
    raw = dot(wq_t[...], q_norm.astype(BF16)).astype(BF16).astype(F32)
    for h in range(2):
        q_own[h] = (finish(raw[h * 96 : h * 96 + 96], column(qh_gain)) * SCALE).astype(BF16)

    for j in range(2):
        here = jnp.logical_and(even, 2 * c + j == y)

        @pl.when(jnp.logical_not(here))
        def _():
            q_copy(j).start()

        @pl.when(here)
        def _():
            q_in[owner] = q_own[j]

    def wait_slot(slot):
        remote(kv_all.at[slot], kv_all.at[slot], sib_send.at[slot], kv_recv.at[slot], sib).wait_recv()

    def ring_copy(slot, way, b, s):
        return remote(kv_all.at[slot], kv_all.at[slot], ring_send.at[way, b, s], kv_recv.at[slot], (up, down)[way])

    def sib_copy(slot):
        return remote(kv_all.at[slot], kv_all.at[slot], sib_send.at[slot], kv_recv.at[slot], sib)

    def attend(slots, blocks, diagonal):
        units = [(slot, qb, qc) for slot in slots for qb in blocks for qc in range(3)]

        def score(unit):
            slot, qb, qc = unit
            keys = (qc + 1) * 256 if diagonal else ROWS
            return dot(k_rows[slot, pl.ds(0, keys), :], q_in[qb, :, pl.ds(qc * 256, 256)])

        ready = [score(unit) for unit in units[:2]]
        for i, (slot, qb, qc) in enumerate(units):
            if i + 2 < len(units):
                ready.append(score(units[i + 2]))
            columns = pl.ds(qc * 256, 256)
            keys = (qc + 1) * 256 if diagonal else ROWS
            weights = jnp.exp2(ready.pop(0))
            if diagonal:
                k_pos = lax.broadcasted_iota(jnp.int32, (keys, 256), 0)
                q_pos = lax.broadcasted_iota(jnp.int32, (keys, 256), 1) + qc * 256
                weights = jnp.where(k_pos <= q_pos, weights, 0.0)
            den[qb, :, columns] += jnp.sum(weights.reshape(keys // 8, 8, 256), axis=0)
            acc[qb, :, columns] += dot(kv_all[slot, pl.ds(96, 64), pl.ds(0, keys)], weights.astype(BF16))

    def plane_of(way, s):
        return lax.rem(z + 8 - s, 8) if way == 0 else lax.rem(z + s, 8)

    def pass_on(s, b):
        @pl.when(jnp.logical_and(s == 0, 2 * c + b != y))
        def _():
            wait_slot(z * 4 + 2 * c + b)

        for way in ((0, 1), (1, 0))[b]:
            limit = 4 if way == b else 3
            slot = plane_of(way, s) * 4 + 2 * c + b

            @pl.when(jnp.logical_and(s >= 1, s <= limit))
            def _():
                wait_slot(slot)

            @pl.when(s < limit)
            def _():
                ring_copy(slot, way, b, s).start()

            @pl.when(jnp.logical_and(jnp.logical_or(s >= 1, way == 0), s <= limit))
            def _():
                sib_copy(slot).start()

    def query_row(qb):
        return jnp.where(qb == 0, c, 3 - c)

    def turn_keys(slot):
        k_rows[slot] = turned(kv_all[slot, pl.ds(0, HEAD), :]).astype(BF16)

    def use_own_plane():
        for b in range(2):
            wait_slot(z * 4 + 2 * (1 - c) + b)
        for yb in range(4):
            turn_keys(z * 4 + yb)

        @pl.loop(0, 2)
        def _(qb):
            row = query_row(qb)

            @pl.loop(0, row)
            def _(yb):
                attend([z * 4 + yb], [qb], False)

            attend([z * 4 + row], [qb], True)

    def use_pair(zb, b):
        wait_slot(zb * 4 + 2 * (1 - c) + b)

        @pl.when(zb < z)
        def _():
            pair = [zb * 4 + b, zb * 4 + 2 + b]
            for slot in pair:
                turn_keys(slot)
            attend(pair, (0, 1), False)

    def back(qb, t):
        return remote(
            o_rows.at[qb, t], att_all.at[4 * x + y], o_send.at[qb, t], o_recv.at[4 * x + y],
            {"sp": z * 4 + query_row(qb), "tp": t},
        )

    def is_me(qb, t):
        return jnp.logical_and(query_row(qb) == y, tp == t)

    def send_back(qb):
        rows = jnp.transpose(acc[qb] / jnp.sum(den[qb], axis=0, keepdims=True)).reshape(8, 2, HALF, VDIM)
        o_rows[qb] = jnp.concatenate([rows[:, 0], rows[:, 1]], axis=2).astype(BF16)
        for t in range(8):
            @pl.when(jnp.logical_not(is_me(qb, t)))
            def _():
                back(qb, t).start()

            @pl.when(is_me(qb, t))
            def _():
                att_all[4 * x + y] = o_rows[qb, t]

    @pl.loop(0, 11)
    def _(turn):
        s, b = turn // 2, lax.rem(turn, 2)
        for k in range(2):
            @pl.when(jnp.logical_and(b == k, turn < 10))
            def _():
                pass_on(s, k)

        for qb in range(2):
            kept = jnp.logical_and(jnp.logical_and(even, 2 * c == y), owner == qb)

            @pl.when(jnp.logical_and(turn == 1, jnp.logical_not(kept)))
            def _():
                remote(q_own.at[0], q_in.at[qb], q_send.at[0], q_recv.at[qb], sib).wait_recv()

        @pl.when(turn == 4)
        def _():
            weights_out.relay_first()

        @pl.when(turn == 6)
        def _():
            weights_out.relay_second()

        @pl.when(turn == 8)
        def _():
            weights_out.relay_far()

        @pl.when(turn == 1)
        def _():
            use_own_plane()

        step, half = (turn - 1) // 2, lax.rem(turn + 1, 2)

        @pl.when(turn >= 3)
        def _():
            @pl.loop(0, jnp.where(step < 4, 2, 1))
            def _(side):
                use_pair(lax.rem(z + 8 + jnp.where(side == 0, -step, step), 8), half)

    for qb in range(2):
        send_back(qb)

    for k in range(1, 8):
        idx = lax.rem(tp + k, 8)
        remote(pool_in.at[0], pool_in.at[idx], p_send.at[k], p_recv.at[idx], sib).wait_recv()
    for offset in (0, -1, 1, 2):
        weights_out.wait_sibling(offset)
    for t in range(8):
        lhs[:, pl.ds(t * 128, 128)] = pool_in[t]

    def out_part(first, part_of):
        columns = pl.ds(part_of * 512, 512)
        return dot(lhs[...], w_all[:, pl.ds(first, 128), columns].reshape(D // 2, 512)), columns

    for part_of in range(4):
        value, columns = out_part(0, part_of)
        total[:, columns] = value

    mine = q_c == c

    @pl.loop(0, 16)
    def _(head):
        @pl.when(jnp.logical_not(jnp.logical_and(mine, head == 4 * x + y)))
        def _():
            remote(att_all.at[0], att_all.at[head], o_send.at[0, 0], o_recv.at[head], sib).wait_recv()

    for t in range(8):
        two = [att_all[2 * t], att_all[2 * t + 1]]
        for h in range(2):
            rows = [value[:, h * 64 : h * 64 + 64] for value in two]
            lhs[pl.ds(h * HALF, HALF), pl.ds(t * 128, 128)] = jnp.concatenate(rows, axis=1)
    for part_of in range(4):
        value, columns = out_part(128, part_of)
        out_ref[:, columns] = (total[:, columns] + value).astype(BF16)

    acts.finish()
    kv_lats.finish()
    q_lats.finish()
    halo.wait_send()
    for j in range(2):
        @pl.when(jnp.logical_not(jnp.logical_and(even, 2 * c + j == y)))
        def _():
            q_copy(j).wait_send()

        @pl.when(2 * c + j != y)
        def _():
            kv_copy(j).wait_send()

    for qb in range(2):
        for t in range(8):
            @pl.when(jnp.logical_not(is_me(qb, t)))
            def _():
                back(qb, t).wait_send()

    for k in range(1, 8):
        pool_copy(k).wait_send()
    weights_out.finish()
    for b in range(2):
        for way in range(2):
            for s in range(4 if way == b else 3):
                ring_copy(0, way, b, s).wait_send()

    @pl.loop(0, 8)
    def _(zb):
        for b in range(2):
            sib_copy(zb * 4 + 2 * c + b).wait_send()


DMA = pltpu.SemaphoreType.DMA


def params(number):
    return pltpu.CompilerParams(collective_id=number, has_side_effects=True, vmem_limit_bytes=60 * 1024 * 1024)


def local(
    activations, in_gain, w_pool_in, pool_gain, w_qlat, w_kvlat, w_krope, qlat_gain, kvlat_gain,
    w_qup, w_kup, w_vup, qhead_gain, khead_gain, w_out_pool, w_out_attn,
):
    tables = [jnp.asarray(t) for t in rotary_tables()]
    gather_sems = [DMA((6,)), DMA((8,)), DMA((8, 2))]
    return pl.pallas_call(
        mixer_kernel,
        name="mixer",
        out_shape=jax.ShapeDtypeStruct((BLOCK, D), BF16),
        in_specs=[VMEM_SPEC] * 20,
        out_specs=VMEM_SPEC,
        scratch_shapes=[
            pltpu.VMEM((8, BLOCK, D), BF16),
            pltpu.VMEM((ROWS, 192), F32),
            pltpu.VMEM((64, ROWS), BF16),
            pltpu.VMEM((8, 64, ROWS), BF16),
            pltpu.VMEM((96, ROWS), BF16),
            pltpu.VMEM((8, 96, ROWS), BF16),
            pltpu.VMEM((HALO + ROWS, 128), F32),
            pltpu.VMEM((HALO, 128), BF16),
            pltpu.VMEM((HALO, 128), BF16),
            pltpu.VMEM((D, 192), BF16),
            pltpu.VMEM((256, KVLAT), BF16),
            pltpu.VMEM((2, HEAD, ROWS), BF16),
            pltpu.VMEM((2, LAT, ROWS), BF16),
            pltpu.VMEM((ROWS, 128), BF16),
            pltpu.VMEM((32, LAT, ROWS), BF16),
            pltpu.VMEM((32, ROWS, HEAD), BF16),
            pltpu.VMEM((2, HEAD, ROWS), BF16),
            pltpu.VMEM((2, VDIM, ROWS), F32),
            pltpu.VMEM((2, 8, ROWS), F32),
            pltpu.VMEM((2, 8, HALF, 128), BF16),
            pltpu.VMEM((16, HALF, 128), BF16),
            pltpu.VMEM((8, BLOCK, 128), BF16),
            pltpu.VMEM((8, 256, D), BF16),
            pltpu.VMEM((BLOCK, D // 2), BF16),
            pltpu.VMEM((BLOCK, D), F32),
            *gather_sems, *gather_sems, *gather_sems, DMA((2,)),
            DMA((2,)), DMA((32,)), DMA((2,)), DMA((2,)), DMA((2, 2, 4)), DMA((32,)), DMA((2, 8)), DMA((16,)),
            DMA((8,)), DMA((8,)), *gather_sems,
        ],
        compiler_params=params(1),
    )(
        activations, in_gain[None, :], w_pool_in, w_qlat.T, w_kvlat.T, w_krope.T, pool_gain[None, :], qlat_gain[None, :],
        kvlat_gain[None, :], w_qup.T, w_kup, w_vup, qhead_gain[None, :], khead_gain[None, :], *tables, w_out_pool, w_out_attn,
    )


def solution(mesh):
    placed = (
        P(("sp", "tp"), None), P(), P(None, "tp"), P("tp"), P(None, "tp"), P(None, "tp"), P(), P(), P(),
        P(None, "tp"), P(None, "tp"), P(None, "tp"), P(), P(), P("tp", None), P("tp", None),
    )
    return jax.shard_map(local, mesh=mesh, in_specs=placed, out_specs=P(("sp", "tp"), None), check_vma=False)
```

```python
import functools
import math

import jax
import jax.numpy as jnp
import numpy as np
from jax import lax
from jax.experimental import pallas as pl
from jax.experimental.pallas import tpu as pltpu
from jax.sharding import PartitionSpec as P

NOPE = 64
ROPE = 32
HEAD = NOPE + ROPE
VDIM = 64
QLAT = 768
KVLAT = 512
EPS = 1e-06
THETA = 10000.0
ROWS = 768
BLOCK = 96
HALF = BLOCK // 2
D = 2048
LAT = 160
HALO = 16
F32 = jnp.float32
BF16 = jnp.bfloat16
MESH = pl.DeviceIdType.MESH
VMEM_SPEC = pl.BlockSpec(memory_space=pltpu.VMEM)
ANY_SPEC = pl.BlockSpec(memory_space=pl.ANY)
SCALE = (1.0 / math.sqrt(HEAD)) * math.log2(math.e)


def dot(a, b):
    return jnp.dot(a, b, preferred_element_type=F32)


def turned(a):
    return jnp.transpose(a.astype(F32))


def column(gain, flat=False):
    row = gain[...][None, :] if flat else gain[...]
    return jnp.transpose(jnp.broadcast_to(row, (8, row.shape[1])))[:, 0:1]


def rotary_tables():
    freq = THETA ** (-np.arange(0, ROPE, 2, dtype=np.float64) / ROPE)
    far = freq[:, None] * (np.arange(128, dtype=np.float64)[None, :] * ROWS)
    near = freq[:, None] * np.arange(ROWS, dtype=np.float64)[None, :]
    return tuple(t.astype(np.float32) for t in (np.cos(far), np.sin(far), np.cos(near), np.sin(near)))


def place():
    sp = lax.axis_index("sp")
    tp = lax.axis_index("tp")
    return sp, tp, tp // 2, lax.rem(tp, 2)


def meet(devices):
    barrier = pltpu.get_barrier_semaphore()
    for device in devices:
        pl.semaphore_signal(barrier, inc=1, device_id=device, device_id_type=MESH)
    pl.semaphore_wait(barrier, len(devices))


def remote(src, dst, send_sem, recv_sem, device):
    return pltpu.make_async_remote_copy(
        src_ref=src, dst_ref=dst, send_sem=send_sem, recv_sem=recv_sem, device_id=device, device_id_type=MESH
    )


class TpGather:
    def __init__(self, own, everything, half, sp, x, c, ring_send, sib_send, recv):
        self.own, self.all, self.half = own, everything, half
        self.x, self.c = x, c
        self.ring_send, self.sib_send, self.recv = ring_send, sib_send, recv
        self.right = {"sp": sp, "tp": lax.rem(x + 1, 4) * 2 + c}
        self.left = {"sp": sp, "tp": lax.rem(x + 3, 4) * 2 + c}
        self.sib = {"sp": sp, "tp": x * 2 + 1 - c}

    def index(self, offset, core):
        return lax.rem(self.x + 4 + offset, 4) * 2 + core

    def piece(self, idx, h):
        return self.all.at[idx, pl.ds(h * self.half, self.half)]

    def copy(self, src, idx, h, send, device):
        return remote(src, self.piece(idx, h), send, self.recv.at[idx, h], device)

    def start(self):
        me = self.index(0, self.c)
        for k, (device, h) in enumerate(((self.right, 0), (self.left, 1), (self.right, 1), (self.left, 0))):
            self.copy(self.own[h], me, h, self.ring_send.at[k], device).start()
        for h in range(2):
            self.copy(self.own[h], me, h, self.sib_send.at[h], self.sib).start()

    def wait_piece(self, idx, h):
        self.copy(self.own[h], idx, h, self.sib_send.at[0], self.sib).wait_recv()

    def got(self, offset, h, slot, onward=None, onward_slot=0):
        idx = self.index(offset, self.c)
        self.wait_piece(idx, h)
        if onward is not None:
            self.copy(self.piece(idx, h), idx, h, self.ring_send.at[onward_slot], onward).start()
        self.copy(self.piece(idx, h), idx, h, self.sib_send.at[slot], self.sib).start()

    def relay_first(self):
        self.got(-1, 0, 2, self.right, 4)
        self.got(1, 1, 3, self.left, 5)

    def relay_second(self):
        self.got(-1, 1, 4)
        self.got(1, 0, 5)

    def relay_far(self):
        self.got(2, 0, 6)
        self.got(2, 1, 7)

    def wait_sibling(self, offset):
        idx = self.index(offset, 1 - self.c)
        for h in range(2):
            self.wait_piece(idx, h)
        return idx

    def finish(self):
        for k in range(6):
            self.copy(self.own[0], 0, 0, self.ring_send.at[k], self.sib).wait_send()
        for k in range(8):
            self.copy(self.own[0], 0, 0, self.sib_send.at[k], self.sib).wait_send()


def mixer_kernel(
    act, in_gain, w_pool_hbm, w_qlat_hbm, w_kvlat_hbm, w_krope_hbm, pool_gain, q_gain, kv_gain, wq_hbm, w_kup_hbm, w_vup_hbm, qh_gain, kh_gain,
    far_cos, far_sin, near_cos, near_sin, w_out_pool, w_out_attn,
    out_ref,
    w_pool, w_lat_t, wq_t, w_up, load_sem,
    act_all, lat_rows, kvl_own, kvl_all, ql_own, ql_all, pool_rows, halo_out, halo_in, w_lat, wkv_t, q_own, kv_own, pool_own,
    kv_all, k_rows, q_in, acc, den, o_rows, att_all, pool_in, w_all, lhs, total,
    a_ring, a_sib, a_recv, k_ring, k_sib, k_recv, l_ring, l_sib, l_recv, halo_sem,
    c_send, kv_recv, q_send, q_recv, ring_send, sib_send, o_send, o_recv, p_send, p_recv, w_ring, w_sib, w_recv,
):
    sp, tp, x, c = place()
    z, y = sp // 4, lax.rem(sp, 4)
    even = lax.rem(y, 2) == 0
    owner = y // 2
    q_c = jnp.where(y < 2, y, 3 - y)

    def device(yy, zz, cc, xx=x):
        return {"sp": zz * 4 + yy, "tp": xx * 2 + cc}

    up = device(y, lax.rem(z + 1, 8), c)
    down = device(y, lax.rem(z + 7, 8), c)
    sib = device(y, z, 1 - c)
    behind = {"sp": lax.rem(sp + 1, 32), "tp": tp}
    before = {"sp": lax.rem(sp + 31, 32), "tp": tp}

    def gather(own, everything, half, *sems):
        return TpGather(own, everything, half, sp, x, c, *sems)

    loads = [
        pltpu.make_async_copy(src, dst, load_sem.at[k])
        for k, (src, dst) in enumerate((
            (w_qlat_hbm, w_lat_t.at[pl.ds(0, 96)]), (w_kvlat_hbm, w_lat_t.at[pl.ds(96, 64)]), (w_krope_hbm, w_lat_t.at[pl.ds(160, 32)]),
            (w_pool_hbm, w_pool), (w_kup_hbm, w_up.at[0]), (w_vup_hbm, w_up.at[1]), (wq_hbm, wq_t),
            (w_out_pool, w_all.at[tp, pl.ds(0, 128)]), (w_out_attn, w_all.at[tp, pl.ds(128, 128)]),
        ))
    ]
    for load in loads:
        load.start()

    acts = gather([act.at[pl.ds(0, HALF)], act.at[pl.ds(HALF, HALF)]], act_all, HALF, a_ring, a_sib, a_recv)
    kv_lats = gather([kvl_own.at[pl.ds(0, 32)], kvl_own.at[pl.ds(32, 32)]], kvl_all, 32, k_ring, k_sib, k_recv)
    q_lats = gather([ql_own.at[pl.ds(0, 48)], ql_own.at[pl.ds(48, 48)]], ql_all, 48, l_ring, l_sib, l_recv)
    weights_out = gather([w_all.at[tp, pl.ds(0, 128)], w_all.at[tp, pl.ds(128, 128)]], w_all, 128, w_ring, w_sib, w_recv)

    friends = [up, down, behind, before]
    for dy in range(4):
        for dc in range(2):
            yy, cc = lax.rem(y + dy, 4), lax.rem(c + dc, 2)
            if dy or dc:
                friends.append(device(yy, z, cc))
    friends += [{"sp": sp, "tp": lax.rem(tp + k, 8)} for k in range(1, 8)]
    for dx in range(1, 4):
        for dy in range(4):
            friends.append(device(lax.rem(y + dy, 4), z, q_c, lax.rem(x + dx, 4)))
    meet(friends)

    acts.start()

    def project(block, idx):
        rows = pl.multiple_of(idx * BLOCK, 32)
        value = block[...].astype(F32)
        factor = lax.rsqrt(jnp.mean(value * value, axis=1, keepdims=True) + EPS)
        normed = (value * factor * in_gain[...]).astype(BF16)
        pool_rows[pl.ds(HALO + rows, BLOCK), :] = dot(normed, w_pool[...]).astype(BF16).astype(F32)
        lat_rows[pl.ds(rows, BLOCK), :] = dot(normed, w_lat[...])

    for load in loads:
        load.wait()
    w_lat[...] = turned(w_lat_t[...]).astype(BF16)
    project(act, tp)
    wkv_t[pl.ds(0, 128), :] = turned(w_up[0]).astype(BF16)
    wkv_t[pl.ds(128, 128), :] = turned(w_up[1]).astype(BF16)
    idx = acts.wait_sibling(0)
    project(act_all.at[idx], idx)
    acts.relay_first()
    acts.relay_second()
    for offset in (-1, 1):
        idx = acts.index(offset, c)
        project(act_all.at[idx], idx)
    for offset in (-1, 1):
        idx = acts.wait_sibling(offset)
        project(act_all.at[idx], idx)
    acts.relay_far()
    idx = acts.index(2, c)
    project(act_all.at[idx], idx)
    idx = acts.wait_sibling(2)
    project(act_all.at[idx], idx)

    lat_t = jnp.transpose(lat_rows[...])
    kvl_own[...] = lat_t[96:160].astype(BF16)
    ql_own[...] = lat_t[0:96].astype(BF16)
    rope_t = lat_t[160:192].astype(BF16).astype(F32)
    halo_out[...] = pool_rows[pl.ds(ROWS, HALO), :].astype(BF16)
    kv_lats.start()
    halo = remote(halo_out, halo_in, halo_sem.at[0], halo_sem.at[1], behind)
    halo.start()
    kvl_all[tp] = kvl_own[...]
    ql_all[tp] = ql_own[...]

    column_of = lax.broadcasted_iota(jnp.int32, (16, 128), 1) == sp
    cos = jnp.sum(jnp.where(column_of, far_cos[...], 0.0), axis=1, keepdims=True)
    sin = jnp.sum(jnp.where(column_of, far_sin[...], 0.0), axis=1, keepdims=True)
    cosine = cos * near_cos[...] - sin * near_sin[...]
    sine = sin * near_cos[...] + cos * near_sin[...]

    kv_lats.relay_first()
    q_lats.start()
    kv_lats.relay_second()
    kv_lats.relay_far()
    for offset in (0, -1, 1, 2):
        kv_lats.wait_sibling(offset)

    def finish(head, gain):
        factor = lax.rsqrt(jnp.sum(head * head, axis=0, keepdims=True) / HEAD + EPS)
        head = head * factor * gain
        lower, upper = head[64:80], head[80:96]
        return jnp.concatenate([head[:64], lower * cosine - upper * sine, upper * cosine + lower * sine], axis=0)

    kv_lat = kvl_all[...].reshape(KVLAT, ROWS).astype(F32)
    kv_norm = kv_lat * lax.rsqrt(jnp.sum(kv_lat * kv_lat, axis=0, keepdims=True) / KVLAT + EPS) * column(kv_gain)
    plain = dot(wkv_t[...], kv_norm.astype(BF16)).astype(BF16)
    for h in range(2):
        joined = jnp.concatenate([plain[h * 64 : h * 64 + 64].astype(F32), rope_t], axis=0)
        kv_own[h, 0:96, :] = finish(joined, column(kh_gain)).astype(BF16)
        kv_own[h, 96:160, :] = plain[128 + h * 64 : 192 + h * 64]

    def kv_copy(j):
        return remote(kv_own.at[j], kv_all.at[sp], c_send.at[j], kv_recv.at[sp], device(2 * c + j, z, owner))

    def q_copy(j):
        return remote(q_own.at[j], q_in.at[owner], q_send.at[j], q_recv.at[owner], device(2 * c + j, z, q_c))

    for j in range(2):
        here = 2 * c + j == y

        @pl.when(jnp.logical_not(here))
        def _():
            kv_copy(j).start()

        @pl.when(here)
        def _():
            kv_all[sp] = kv_own[j]

    def pool_copy(k):
        to = lax.rem(tp + k, 8)
        rows = pl.multiple_of(to * BLOCK, 32)
        return remote(pool_own.at[pl.ds(rows, BLOCK)], pool_in.at[tp], p_send.at[k], p_recv.at[tp], {"sp": sp, "tp": to})

    def mix_pool():
        halo.wait_recv()
        pool_rows[pl.ds(0, HALO), :] = jnp.where(sp > 0, halo_in[...].astype(F32), 0.0)
        window = jnp.left_shift(jnp.int32(2), tp // 2)
        summed = jnp.zeros((ROWS, 128), F32)
        for lag in range(16):
            summed = summed + jnp.where(lag < window, pool_rows[pl.ds(HALO - lag, ROWS), :], 0.0)
        position = sp * ROWS + lax.broadcasted_iota(jnp.int32, (ROWS, 128), 0)
        divisor = jnp.minimum(position + 1, window).astype(F32)
        pooled = summed / divisor - pool_rows[pl.ds(HALO, ROWS), :]
        pool_own[...] = (pooled * pool_gain[...]).astype(BF16)
        for k in range(1, 8):
            pool_copy(k).start()
        pool_in[tp] = pool_own[pl.ds(pl.multiple_of(tp * BLOCK, 32), BLOCK), :]
        acc[...] = jnp.zeros_like(acc)
        den[...] = jnp.zeros_like(den)

    q_lats.relay_first()
    q_lats.relay_second()
    mix_pool()
    q_lats.relay_far()
    for offset in (0, -1, 1, 2):
        q_lats.wait_sibling(offset)
    weights_out.start()
    def ask():
        q_lat = ql_all[...].reshape(QLAT, ROWS).astype(F32)
        q_norm = q_lat * lax.rsqrt(jnp.sum(q_lat * q_lat, axis=0, keepdims=True) / QLAT + EPS) * column(q_gain, True)
        raw = dot(wq_t[...], q_norm.astype(BF16)).astype(BF16).astype(F32)
        for h in range(2):
            q_own[h] = (finish(raw[h * 96 : h * 96 + 96], column(qh_gain)) * SCALE).astype(BF16)

        for j in range(2):
            here = jnp.logical_and(even, 2 * c + j == y)

            @pl.when(jnp.logical_not(here))
            def _():
                q_copy(j).start()

            @pl.when(here)
            def _():
                q_in[owner] = q_own[j]

    def wait_slot(slot):
        remote(kv_all.at[slot], kv_all.at[slot], sib_send.at[slot], kv_recv.at[slot], sib).wait_recv()

    def ring_copy(slot, way, b, s):
        return remote(kv_all.at[slot], kv_all.at[slot], ring_send.at[way, b, s], kv_recv.at[slot], (up, down)[way])

    def sib_copy(slot):
        return remote(kv_all.at[slot], kv_all.at[slot], sib_send.at[slot], kv_recv.at[slot], sib)

    def attend(slots, blocks, diagonal):
        units = [(slot, qb, qc) for slot in slots for qb in blocks for qc in range(3)]

        def score(unit):
            slot, qb, qc = unit
            keys = (qc + 1) * 256 if diagonal else ROWS
            return dot(k_rows[slot, pl.ds(0, keys), :], q_in[qb, :, pl.ds(qc * 256, 256)])

        ready = [score(unit) for unit in units[:2]]
        for i, (slot, qb, qc) in enumerate(units):
            if i + 2 < len(units):
                ready.append(score(units[i + 2]))
            columns = pl.ds(qc * 256, 256)
            keys = (qc + 1) * 256 if diagonal else ROWS
            weights = jnp.exp2(ready.pop(0))
            if diagonal:
                k_pos = lax.broadcasted_iota(jnp.int32, (keys, 256), 0)
                q_pos = lax.broadcasted_iota(jnp.int32, (keys, 256), 1) + qc * 256
                weights = jnp.where(k_pos <= q_pos, weights, 0.0)
            den[qb, :, columns] += jnp.sum(weights.reshape(keys // 8, 8, 256), axis=0)
            acc[qb, :, columns] += dot(kv_all[slot, pl.ds(96, 64), pl.ds(0, keys)], weights.astype(BF16))

    def plane_of(way, s):
        return lax.rem(z + 8 - s, 8) if way == 0 else lax.rem(z + s, 8)

    def pass_on(s, b):
        @pl.when(jnp.logical_and(s == 0, 2 * c + b != y))
        def _():
            wait_slot(z * 4 + 2 * c + b)

        for way in ((0, 1), (1, 0))[b]:
            limit = 4 if way == b else 3
            slot = plane_of(way, s) * 4 + 2 * c + b

            @pl.when(jnp.logical_and(s >= 1, s <= limit))
            def _():
                wait_slot(slot)

            @pl.when(s < limit)
            def _():
                ring_copy(slot, way, b, s).start()

            @pl.when(jnp.logical_and(jnp.logical_or(s >= 1, way == 0), s <= limit))
            def _():
                sib_copy(slot).start()

    def query_row(qb):
        return jnp.where(qb == 0, c, 3 - c)

    def turn_keys(slot):
        k_rows[slot] = turned(kv_all[slot, pl.ds(0, HEAD), :]).astype(BF16)

    def use_own_plane():
        for b in range(2):
            wait_slot(z * 4 + 2 * (1 - c) + b)
        for yb in range(4):
            turn_keys(z * 4 + yb)

        @pl.loop(0, 2)
        def _(qb):
            row = query_row(qb)

            @pl.loop(0, row)
            def _(yb):
                attend([z * 4 + yb], [qb], False)

            attend([z * 4 + row], [qb], True)

    def use_pair(zb, b):
        wait_slot(zb * 4 + 2 * (1 - c) + b)

        @pl.when(zb < z)
        def _():
            pair = [zb * 4 + b, zb * 4 + 2 + b]
            for slot in pair:
                turn_keys(slot)
            attend(pair, (0, 1), False)

    def back(qb, t):
        return remote(
            o_rows.at[qb, t], att_all.at[4 * x + y], o_send.at[qb, t], o_recv.at[4 * x + y],
            {"sp": z * 4 + query_row(qb), "tp": t},
        )

    def is_me(qb, t):
        return jnp.logical_and(query_row(qb) == y, tp == t)

    def send_back(qb):
        rows = jnp.transpose(acc[qb] / jnp.sum(den[qb], axis=0, keepdims=True)).reshape(8, 2, HALF, VDIM)
        o_rows[qb] = jnp.concatenate([rows[:, 0], rows[:, 1]], axis=2).astype(BF16)
        for t in range(8):
            @pl.when(jnp.logical_not(is_me(qb, t)))
            def _():
                back(qb, t).start()

            @pl.when(is_me(qb, t))
            def _():
                att_all[4 * x + y] = o_rows[qb, t]

    @pl.loop(0, 11)
    def _(turn):
        s, b = turn // 2, lax.rem(turn, 2)
        for k in range(2):
            @pl.when(jnp.logical_and(b == k, turn < 10))
            def _():
                pass_on(s, k)

        @pl.when(turn == 1)
        def _():
            ask()

        for qb in range(2):
            kept = jnp.logical_and(jnp.logical_and(even, 2 * c == y), owner == qb)

            @pl.when(jnp.logical_and(turn == 1, jnp.logical_not(kept)))
            def _():
                remote(q_own.at[0], q_in.at[qb], q_send.at[0], q_recv.at[qb], sib).wait_recv()

        @pl.when(turn == 4)
        def _():
            weights_out.relay_first()

        @pl.when(turn == 6)
        def _():
            weights_out.relay_second()

        @pl.when(turn == 8)
        def _():
            weights_out.relay_far()

        @pl.when(turn == 1)
        def _():
            use_own_plane()

        step, half = (turn - 1) // 2, lax.rem(turn + 1, 2)

        @pl.when(turn >= 3)
        def _():
            @pl.loop(0, jnp.where(step < 4, 2, 1))
            def _(side):
                use_pair(lax.rem(z + 8 + jnp.where(side == 0, -step, step), 8), half)

    for qb in range(2):
        send_back(qb)

    for k in range(1, 8):
        idx = lax.rem(tp + k, 8)
        remote(pool_in.at[0], pool_in.at[idx], p_send.at[k], p_recv.at[idx], sib).wait_recv()
    for offset in (0, -1, 1, 2):
        weights_out.wait_sibling(offset)
    for t in range(8):
        lhs[:, pl.ds(t * 128, 128)] = pool_in[t]

    def out_part(first, part_of):
        columns = pl.ds(part_of * 512, 512)
        return dot(lhs[...], w_all[:, pl.ds(first, 128), columns].reshape(D // 2, 512)), columns

    for part_of in range(4):
        value, columns = out_part(0, part_of)
        total[:, columns] = value

    mine = q_c == c

    @pl.loop(0, 16)
    def _(head):
        @pl.when(jnp.logical_not(jnp.logical_and(mine, head == 4 * x + y)))
        def _():
            remote(att_all.at[0], att_all.at[head], o_send.at[0, 0], o_recv.at[head], sib).wait_recv()

    for t in range(8):
        two = [att_all[2 * t], att_all[2 * t + 1]]
        for h in range(2):
            rows = [value[:, h * 64 : h * 64 + 64] for value in two]
            lhs[pl.ds(h * HALF, HALF), pl.ds(t * 128, 128)] = jnp.concatenate(rows, axis=1)
    for part_of in range(4):
        value, columns = out_part(128, part_of)
        out_ref[:, columns] = (total[:, columns] + value).astype(BF16)

    acts.finish()
    kv_lats.finish()
    q_lats.finish()
    halo.wait_send()
    for j in range(2):
        @pl.when(jnp.logical_not(jnp.logical_and(even, 2 * c + j == y)))
        def _():
            q_copy(j).wait_send()

        @pl.when(2 * c + j != y)
        def _():
            kv_copy(j).wait_send()

    for qb in range(2):
        for t in range(8):
            @pl.when(jnp.logical_not(is_me(qb, t)))
            def _():
                back(qb, t).wait_send()

    for k in range(1, 8):
        pool_copy(k).wait_send()
    weights_out.finish()
    for b in range(2):
        for way in range(2):
            for s in range(4 if way == b else 3):
                ring_copy(0, way, b, s).wait_send()

    @pl.loop(0, 8)
    def _(zb):
        for b in range(2):
            sib_copy(zb * 4 + 2 * c + b).wait_send()


DMA = pltpu.SemaphoreType.DMA


def params(number):
    return pltpu.CompilerParams(collective_id=number, has_side_effects=True, vmem_limit_bytes=60 * 1024 * 1024)


def local(
    activations, in_gain, w_pool_in, pool_gain, w_qlat, w_kvlat, w_krope, qlat_gain, kvlat_gain,
    w_qup, w_kup, w_vup, qhead_gain, khead_gain, w_out_pool, w_out_attn,
):
    tables = [jnp.asarray(t) for t in rotary_tables()]
    gather_sems = [DMA((6,)), DMA((8,)), DMA((8, 2))]
    return pl.pallas_call(
        mixer_kernel,
        name="mixer",
        out_shape=jax.ShapeDtypeStruct((BLOCK, D), BF16),
        in_specs=[ANY_SPEC if k in (2, 3, 4, 5, 9, 10, 11, 18, 19) else VMEM_SPEC for k in range(20)],
        out_specs=VMEM_SPEC,
        scratch_shapes=[
            pltpu.VMEM((D, 128), BF16),
            pltpu.VMEM((192, D), BF16),
            pltpu.VMEM((192, QLAT), BF16),
            pltpu.VMEM((2, KVLAT, 128), BF16),
            DMA((9,)),
            pltpu.VMEM((8, BLOCK, D), BF16),
            pltpu.VMEM((ROWS, 192), F32),
            pltpu.VMEM((64, ROWS), BF16),
            pltpu.VMEM((8, 64, ROWS), BF16),
            pltpu.VMEM((96, ROWS), BF16),
            pltpu.VMEM((8, 96, ROWS), BF16),
            pltpu.VMEM((HALO + ROWS, 128), F32),
            pltpu.VMEM((HALO, 128), BF16),
            pltpu.VMEM((HALO, 128), BF16),
            pltpu.VMEM((D, 192), BF16),
            pltpu.VMEM((256, KVLAT), BF16),
            pltpu.VMEM((2, HEAD, ROWS), BF16),
            pltpu.VMEM((2, LAT, ROWS), BF16),
            pltpu.VMEM((ROWS, 128), BF16),
            pltpu.VMEM((32, LAT, ROWS), BF16),
            pltpu.VMEM((32, ROWS, HEAD), BF16),
            pltpu.VMEM((2, HEAD, ROWS), BF16),
            pltpu.VMEM((2, VDIM, ROWS), F32),
            pltpu.VMEM((2, 8, ROWS), F32),
            pltpu.VMEM((2, 8, HALF, 128), BF16),
            pltpu.VMEM((16, HALF, 128), BF16),
            pltpu.VMEM((8, BLOCK, 128), BF16),
            pltpu.VMEM((8, 256, D), BF16),
            pltpu.VMEM((BLOCK, D // 2), BF16),
            pltpu.VMEM((BLOCK, D), F32),
            *gather_sems, *gather_sems, *gather_sems, DMA((2,)),
            DMA((2,)), DMA((32,)), DMA((2,)), DMA((2,)), DMA((2, 2, 4)), DMA((32,)), DMA((2, 8)), DMA((16,)),
            DMA((8,)), DMA((8,)), *gather_sems,
        ],
        compiler_params=params(1),
    )(
        activations, in_gain[None, :], w_pool_in, w_qlat.T, w_kvlat.T, w_krope.T, pool_gain[None, :], qlat_gain,
        kvlat_gain[None, :], w_qup.T, w_kup, w_vup, qhead_gain[None, :], khead_gain[None, :], *tables, w_out_pool, w_out_attn,
    )


def solution(mesh):
    placed = (
        P(("sp", "tp"), None), P(), P(None, "tp"), P("tp"), P(None, "tp"), P(None, "tp"), P(), P(), P(),
        P(None, "tp"), P(None, "tp"), P(None, "tp"), P(), P(), P("tp", None), P("tp", None),
    )
    return jax.shard_map(local, mesh=mesh, in_specs=placed, out_specs=P(("sp", "tp"), None), check_vma=False)
```

```python
import functools
import math

import jax
import jax.numpy as jnp
import numpy as np
from jax import lax
from jax.experimental import pallas as pl
from jax.experimental.pallas import tpu as pltpu
from jax.sharding import PartitionSpec as P

NOPE = 64
ROPE = 32
HEAD = NOPE + ROPE
VDIM = 64
QLAT = 768
KVLAT = 512
EPS = 1e-06
THETA = 10000.0
ROWS = 768
BLOCK = 96
HALF = BLOCK // 2
D = 2048
LAT = 160
HALO = 16
F32 = jnp.float32
BF16 = jnp.bfloat16
MESH = pl.DeviceIdType.MESH
VMEM_SPEC = pl.BlockSpec(memory_space=pltpu.VMEM)
ANY_SPEC = pl.BlockSpec(memory_space=pl.ANY)
SCALE = (1.0 / math.sqrt(HEAD)) * math.log2(math.e)


def dot(a, b):
    return jnp.dot(a, b, preferred_element_type=F32)


def turned(a):
    return jnp.transpose(a.astype(F32))


def column(gain, flat=False):
    row = gain[...][None, :] if flat else gain[...]
    return jnp.transpose(jnp.broadcast_to(row, (8, row.shape[1])))[:, 0:1]


def rotary_tables():
    freq = THETA ** (-np.arange(0, ROPE, 2, dtype=np.float64) / ROPE)
    far = freq[:, None] * (np.arange(128, dtype=np.float64)[None, :] * ROWS)
    near = freq[:, None] * np.arange(ROWS, dtype=np.float64)[None, :]
    return tuple(t.astype(np.float32) for t in (np.cos(far), np.sin(far), np.cos(near), np.sin(near)))


def place():
    sp = lax.axis_index("sp")
    tp = lax.axis_index("tp")
    return sp, tp, tp // 2, lax.rem(tp, 2)


def meet(devices):
    barrier = pltpu.get_barrier_semaphore()
    for device in devices:
        pl.semaphore_signal(barrier, inc=1, device_id=device, device_id_type=MESH)
    pl.semaphore_wait(barrier, len(devices))


def remote(src, dst, send_sem, recv_sem, device):
    return pltpu.make_async_remote_copy(
        src_ref=src, dst_ref=dst, send_sem=send_sem, recv_sem=recv_sem, device_id=device, device_id_type=MESH
    )


class TpGather:
    def __init__(self, own, everything, half, sp, x, c, ring_send, sib_send, recv):
        self.own, self.all, self.half = own, everything, half
        self.x, self.c = x, c
        self.ring_send, self.sib_send, self.recv = ring_send, sib_send, recv
        self.right = {"sp": sp, "tp": lax.rem(x + 1, 4) * 2 + c}
        self.left = {"sp": sp, "tp": lax.rem(x + 3, 4) * 2 + c}
        self.sib = {"sp": sp, "tp": x * 2 + 1 - c}

    def index(self, offset, core):
        return lax.rem(self.x + 4 + offset, 4) * 2 + core

    def piece(self, idx, h):
        return self.all.at[idx, pl.ds(h * self.half, self.half)]

    def copy(self, src, idx, h, send, device):
        return remote(src, self.piece(idx, h), send, self.recv.at[idx, h], device)

    def start(self):
        me = self.index(0, self.c)
        for k, (device, h) in enumerate(((self.right, 0), (self.left, 1), (self.right, 1), (self.left, 0))):
            self.copy(self.own[h], me, h, self.ring_send.at[k], device).start()
        for h in range(2):
            self.copy(self.own[h], me, h, self.sib_send.at[h], self.sib).start()

    def wait_piece(self, idx, h):
        self.copy(self.own[h], idx, h, self.sib_send.at[0], self.sib).wait_recv()

    def got(self, offset, h, slot, onward=None, onward_slot=0):
        idx = self.index(offset, self.c)
        self.wait_piece(idx, h)
        if onward is not None:
            self.copy(self.piece(idx, h), idx, h, self.ring_send.at[onward_slot], onward).start()
        self.copy(self.piece(idx, h), idx, h, self.sib_send.at[slot], self.sib).start()

    def relay_first(self):
        self.got(-1, 0, 2, self.right, 4)
        self.got(1, 1, 3, self.left, 5)

    def relay_second(self):
        self.got(-1, 1, 4)
        self.got(1, 0, 5)

    def relay_far(self):
        self.got(2, 0, 6)
        self.got(2, 1, 7)

    def wait_sibling(self, offset):
        idx = self.index(offset, 1 - self.c)
        for h in range(2):
            self.wait_piece(idx, h)
        return idx

    def finish(self):
        for k in range(6):
            self.copy(self.own[0], 0, 0, self.ring_send.at[k], self.sib).wait_send()
        for k in range(8):
            self.copy(self.own[0], 0, 0, self.sib_send.at[k], self.sib).wait_send()


def mixer_kernel(
    act, in_gain, w_pool_hbm, w_qlat_hbm, w_kvlat_hbm, w_krope_hbm, pool_gain, q_gain, kv_gain, wq_hbm, w_kup_hbm, w_vup_hbm, qh_gain, kh_gain,
    far_cos, far_sin, near_cos, near_sin, w_out_pool, w_out_attn,
    out_ref,
    w_pool, w_lat_t, wq_t, w_up, load_sem,
    act_all, lat_rows, kvl_own, kvl_all, ql_own, ql_all, pool_rows, halo_out, halo_in, w_lat, wkv_t, q_own, kv_own, pool_own,
    kv_all, k_rows, q_in, acc, den, o_rows, att_all, pool_in, w_all, lhs, total,
    a_ring, a_sib, a_recv, k_ring, k_sib, k_recv, l_ring, l_sib, l_recv, halo_sem,
    c_send, kv_recv, q_send, q_recv, ring_send, sib_send, o_send, o_recv, p_send, p_recv, w_ring, w_sib, w_recv,
):
    sp, tp, x, c = place()
    z, y = sp // 4, lax.rem(sp, 4)
    even = lax.rem(y, 2) == 0
    owner = y // 2
    q_c = jnp.where(y < 2, y, 3 - y)

    def device(yy, zz, cc, xx=x):
        return {"sp": zz * 4 + yy, "tp": xx * 2 + cc}

    up = device(y, lax.rem(z + 1, 8), c)
    down = device(y, lax.rem(z + 7, 8), c)
    sib = device(y, z, 1 - c)
    behind = {"sp": lax.rem(sp + 1, 32), "tp": tp}
    before = {"sp": lax.rem(sp + 31, 32), "tp": tp}

    def gather(own, everything, half, *sems):
        return TpGather(own, everything, half, sp, x, c, *sems)

    loads = [
        pltpu.make_async_copy(src, dst, load_sem.at[k])
        for k, (src, dst) in enumerate((
            (w_qlat_hbm, w_lat_t.at[pl.ds(0, 96)]), (w_kvlat_hbm, w_lat_t.at[pl.ds(96, 64)]), (w_krope_hbm, w_lat_t.at[pl.ds(160, 32)]),
            (w_pool_hbm, w_pool), (w_kup_hbm, w_up.at[0]), (w_vup_hbm, w_up.at[1]), (wq_hbm, wq_t),
            (w_out_pool, w_all.at[tp, pl.ds(0, 128)]), (w_out_attn, w_all.at[tp, pl.ds(128, 128)]),
        ))
    ]
    for load in loads:
        load.start()

    acts = gather([act.at[pl.ds(0, HALF)], act.at[pl.ds(HALF, HALF)]], act_all, HALF, a_ring, a_sib, a_recv)
    kv_lats = gather([kvl_own.at[pl.ds(0, 32)], kvl_own.at[pl.ds(32, 32)]], kvl_all, 32, k_ring, k_sib, k_recv)
    q_lats = gather([ql_own.at[pl.ds(0, 48)], ql_own.at[pl.ds(48, 48)]], ql_all, 48, l_ring, l_sib, l_recv)
    weights_out = gather([w_all.at[tp, pl.ds(0, 128)], w_all.at[tp, pl.ds(128, 128)]], w_all, 128, w_ring, w_sib, w_recv)

    friends = [up, down, behind, before]
    for dy in range(4):
        for dc in range(2):
            yy, cc = lax.rem(y + dy, 4), lax.rem(c + dc, 2)
            if dy or dc:
                friends.append(device(yy, z, cc))
    friends += [{"sp": sp, "tp": lax.rem(tp + k, 8)} for k in range(1, 8)]
    for dx in range(1, 4):
        for dy in range(4):
            friends.append(device(lax.rem(y + dy, 4), z, q_c, lax.rem(x + dx, 4)))
    meet(friends)

    acts.start()

    def project(block, idx):
        rows = pl.multiple_of(idx * BLOCK, 32)
        value = block[...].astype(F32)
        factor = lax.rsqrt(jnp.mean(value * value, axis=1, keepdims=True) + EPS)
        normed = (value * factor * in_gain[...]).astype(BF16)
        pool_rows[pl.ds(HALO + rows, BLOCK), :] = dot(normed, w_pool[...]).astype(BF16).astype(F32)
        lat_rows[pl.ds(rows, BLOCK), :] = dot(normed, w_lat[...])

    for load in loads:
        load.wait()
    w_lat[...] = turned(w_lat_t[...]).astype(BF16)
    project(act, tp)
    wkv_t[pl.ds(0, 128), :] = turned(w_up[0]).astype(BF16)
    wkv_t[pl.ds(128, 128), :] = turned(w_up[1]).astype(BF16)
    idx = acts.wait_sibling(0)
    project(act_all.at[idx], idx)
    acts.relay_first()
    acts.relay_second()
    for offset in (-1, 1):
        idx = acts.index(offset, c)
        project(act_all.at[idx], idx)
    for offset in (-1, 1):
        idx = acts.wait_sibling(offset)
        project(act_all.at[idx], idx)
    acts.relay_far()
    idx = acts.index(2, c)
    project(act_all.at[idx], idx)
    idx = acts.wait_sibling(2)
    project(act_all.at[idx], idx)

    lat_t = jnp.transpose(lat_rows[...])
    kvl_own[...] = lat_t[96:160].astype(BF16)
    ql_own[...] = lat_t[0:96].astype(BF16)
    rope_t = lat_t[160:192].astype(BF16).astype(F32)
    halo_out[...] = pool_rows[pl.ds(ROWS, HALO), :].astype(BF16)
    kv_lats.start()
    halo = remote(halo_out, halo_in, halo_sem.at[0], halo_sem.at[1], behind)
    halo.start()
    kvl_all[tp] = kvl_own[...]
    ql_all[tp] = ql_own[...]

    column_of = lax.broadcasted_iota(jnp.int32, (16, 128), 1) == sp
    cos = jnp.sum(jnp.where(column_of, far_cos[...], 0.0), axis=1, keepdims=True)
    sin = jnp.sum(jnp.where(column_of, far_sin[...], 0.0), axis=1, keepdims=True)
    cosine = cos * near_cos[...] - sin * near_sin[...]
    sine = sin * near_cos[...] + cos * near_sin[...]

    kv_lats.relay_first()
    q_lats.start()
    kv_lats.relay_second()
    kv_lats.relay_far()
    for offset in (0, -1, 1, 2):
        kv_lats.wait_sibling(offset)

    def finish(head, gain):
        factor = lax.rsqrt(jnp.sum(head * head, axis=0, keepdims=True) / HEAD + EPS)
        head = head * factor * gain
        lower, upper = head[64:80], head[80:96]
        return jnp.concatenate([head[:64], lower * cosine - upper * sine, upper * cosine + lower * sine], axis=0)

    kv_lat = kvl_all[...].reshape(KVLAT, ROWS).astype(F32)
    kv_norm = kv_lat * lax.rsqrt(jnp.sum(kv_lat * kv_lat, axis=0, keepdims=True) / KVLAT + EPS) * column(kv_gain)
    plain = dot(wkv_t[...], kv_norm.astype(BF16)).astype(BF16)
    for h in range(2):
        joined = jnp.concatenate([plain[h * 64 : h * 64 + 64].astype(F32), rope_t], axis=0)
        kv_own[h, 0:96, :] = finish(joined, column(kh_gain)).astype(BF16)
        kv_own[h, 96:160, :] = plain[128 + h * 64 : 192 + h * 64]

    def kv_copy(j):
        return remote(kv_own.at[j], kv_all.at[sp], c_send.at[j], kv_recv.at[sp], device(2 * c + j, z, owner))

    def q_copy(j):
        return remote(q_own.at[j], q_in.at[owner], q_send.at[j], q_recv.at[owner], device(2 * c + j, z, q_c))

    for j in range(2):
        here = 2 * c + j == y

        @pl.when(jnp.logical_not(here))
        def _():
            kv_copy(j).start()

        @pl.when(here)
        def _():
            kv_all[sp] = kv_own[j]

    def pool_copy(k):
        to = lax.rem(tp + k, 8)
        rows = pl.multiple_of(to * BLOCK, 32)
        return remote(pool_own.at[pl.ds(rows, BLOCK)], pool_in.at[tp], p_send.at[k], p_recv.at[tp], {"sp": sp, "tp": to})

    def mix_pool():
        halo.wait_recv()
        pool_rows[pl.ds(0, HALO), :] = jnp.where(sp > 0, halo_in[...].astype(F32), 0.0)
        window = jnp.left_shift(jnp.int32(2), tp // 2)
        summed = jnp.zeros((ROWS, 128), F32)
        for lag in range(16):
            summed = summed + jnp.where(lag < window, pool_rows[pl.ds(HALO - lag, ROWS), :], 0.0)
        position = sp * ROWS + lax.broadcasted_iota(jnp.int32, (ROWS, 128), 0)
        divisor = jnp.minimum(position + 1, window).astype(F32)
        pooled = summed / divisor - pool_rows[pl.ds(HALO, ROWS), :]
        pool_own[...] = (pooled * pool_gain[...]).astype(BF16)
        for k in range(1, 8):
            pool_copy(k).start()
        pool_in[tp] = pool_own[pl.ds(pl.multiple_of(tp * BLOCK, 32), BLOCK), :]
        acc[...] = jnp.zeros_like(acc)
        den[...] = jnp.zeros_like(den)

    q_lats.relay_first()
    q_lats.relay_second()
    mix_pool()
    q_lats.relay_far()
    for offset in (0, -1, 1, 2):
        q_lats.wait_sibling(offset)
    weights_out.start()
    def ask():
        q_lat = ql_all[...].reshape(QLAT, ROWS).astype(F32)
        q_norm = q_lat * lax.rsqrt(jnp.sum(q_lat * q_lat, axis=0, keepdims=True) / QLAT + EPS) * column(q_gain, True)
        raw = dot(wq_t[...], q_norm.astype(BF16)).astype(BF16).astype(F32)
        for h in range(2):
            q_own[h] = (finish(raw[h * 96 : h * 96 + 96], column(qh_gain)) * SCALE).astype(BF16)

        for j in range(2):
            here = jnp.logical_and(even, 2 * c + j == y)

            @pl.when(jnp.logical_not(here))
            def _():
                q_copy(j).start()

            @pl.when(here)
            def _():
                q_in[owner] = q_own[j]

    def wait_slot(slot):
        remote(kv_all.at[slot], kv_all.at[slot], sib_send.at[slot], kv_recv.at[slot], sib).wait_recv()

    def ring_copy(slot, way, b, s):
        return remote(kv_all.at[slot], kv_all.at[slot], ring_send.at[way, b, s], kv_recv.at[slot], (up, down)[way])

    def sib_copy(slot):
        return remote(kv_all.at[slot], kv_all.at[slot], sib_send.at[slot], kv_recv.at[slot], sib)

    def attend(slots, blocks, diagonal):
        units = [(slot, qb, qc) for slot in slots for qb in blocks for qc in range(3)]

        def score(unit):
            slot, qb, qc = unit
            keys = (qc + 1) * 256 if diagonal else ROWS
            return dot(k_rows[slot, pl.ds(0, keys), :], q_in[qb, :, pl.ds(qc * 256, 256)])

        ready = [score(unit) for unit in units[:2]]
        for i, (slot, qb, qc) in enumerate(units):
            if i + 2 < len(units):
                ready.append(score(units[i + 2]))
            columns = pl.ds(qc * 256, 256)
            keys = (qc + 1) * 256 if diagonal else ROWS
            weights = jnp.exp2(ready.pop(0))
            if diagonal:
                k_pos = lax.broadcasted_iota(jnp.int32, (keys, 256), 0)
                q_pos = lax.broadcasted_iota(jnp.int32, (keys, 256), 1) + qc * 256
                weights = jnp.where(k_pos <= q_pos, weights, 0.0)
            den[qb, :, columns] += jnp.sum(weights.reshape(keys // 8, 8, 256), axis=0)
            acc[qb, :, columns] += dot(kv_all[slot, pl.ds(96, 64), pl.ds(0, keys)], weights.astype(BF16))

    def plane_of(way, s):
        return lax.rem(z + 8 - s, 8) if way == 0 else lax.rem(z + s, 8)

    def pass_on(s, b):
        @pl.when(jnp.logical_and(s == 0, 2 * c + b != y))
        def _():
            wait_slot(z * 4 + 2 * c + b)

        for way in ((0, 1), (1, 0))[b]:
            limit = 4 if way == b else 3
            slot = plane_of(way, s) * 4 + 2 * c + b

            @pl.when(jnp.logical_and(s >= 1, s <= limit))
            def _():
                wait_slot(slot)

            @pl.when(s < limit)
            def _():
                ring_copy(slot, way, b, s).start()

            @pl.when(jnp.logical_and(jnp.logical_or(s >= 1, way == 0), s <= limit))
            def _():
                sib_copy(slot).start()

    def query_row(qb):
        return jnp.where(qb == 0, c, 3 - c)

    def turn_keys(slot):
        k_rows[slot] = turned(kv_all[slot, pl.ds(0, HEAD), :]).astype(BF16)

    def use_own_plane():
        for b in range(2):
            wait_slot(z * 4 + 2 * (1 - c) + b)
        for yb in range(4):
            turn_keys(z * 4 + yb)

        @pl.loop(0, 2)
        def _(qb):
            row = query_row(qb)

            @pl.loop(0, row)
            def _(yb):
                attend([z * 4 + yb], [qb], False)

            attend([z * 4 + row], [qb], True)

    def use_pair(zb, b):
        wait_slot(zb * 4 + 2 * (1 - c) + b)

        @pl.when(zb < z)
        def _():
            pair = [zb * 4 + b, zb * 4 + 2 + b]
            for slot in pair:
                turn_keys(slot)
            attend(pair, (0, 1), False)

    def back(qb, t):
        return remote(
            o_rows.at[qb, t], att_all.at[4 * x + y], o_send.at[qb, t], o_recv.at[4 * x + y],
            {"sp": z * 4 + query_row(qb), "tp": t},
        )

    def is_me(qb, t):
        return jnp.logical_and(query_row(qb) == y, tp == t)

    def send_back(qb):
        rows = jnp.transpose(acc[qb] / jnp.sum(den[qb], axis=0, keepdims=True)).reshape(8, 2, HALF, VDIM)
        o_rows[qb] = jnp.concatenate([rows[:, 0], rows[:, 1]], axis=2).astype(BF16)
        for t in range(8):
            @pl.when(jnp.logical_not(is_me(qb, t)))
            def _():
                back(qb, t).start()

            @pl.when(is_me(qb, t))
            def _():
                att_all[4 * x + y] = o_rows[qb, t]

    @pl.loop(0, 11)
    def _(turn):
        s, b = turn // 2, lax.rem(turn, 2)
        step, half = (turn - 1) // 2, lax.rem(turn + 1, 2)

        @pl.when(turn >= 3)
        def _():
            @pl.loop(0, jnp.where(step < 4, 2, 1))
            def _(side):
                use_pair(lax.rem(z + 8 + jnp.where(side == 0, -step, step), 8), half)

        for k in range(2):
            @pl.when(jnp.logical_and(b == k, turn < 9))
            def _():
                pass_on(s, k)

        @pl.when(turn == 1)
        def _():
            ask()

        for qb in range(2):
            kept = jnp.logical_and(jnp.logical_and(even, 2 * c == y), owner == qb)

            @pl.when(jnp.logical_and(turn == 1, jnp.logical_not(kept)))
            def _():
                remote(q_own.at[0], q_in.at[qb], q_send.at[0], q_recv.at[qb], sib).wait_recv()

        @pl.when(turn == 4)
        def _():
            weights_out.relay_first()

        @pl.when(turn == 6)
        def _():
            weights_out.relay_second()

        @pl.when(turn == 8)
        def _():
            weights_out.relay_far()

        @pl.when(turn == 1)
        def _():
            use_own_plane()

        @pl.when(turn == 8)
        def _():
            pass_on(s, 1)

    for qb in range(2):
        send_back(qb)

    for k in range(1, 8):
        idx = lax.rem(tp + k, 8)
        remote(pool_in.at[0], pool_in.at[idx], p_send.at[k], p_recv.at[idx], sib).wait_recv()
    for offset in (0, -1, 1, 2):
        weights_out.wait_sibling(offset)
    for t in range(8):
        lhs[:, pl.ds(t * 128, 128)] = pool_in[t]

    def out_part(first, part_of):
        columns = pl.ds(part_of * 512, 512)
        return dot(lhs[...], w_all[:, pl.ds(first, 128), columns].reshape(D // 2, 512)), columns

    for part_of in range(4):
        value, columns = out_part(0, part_of)
        total[:, columns] = value

    mine = q_c == c

    @pl.loop(0, 16)
    def _(head):
        @pl.when(jnp.logical_not(jnp.logical_and(mine, head == 4 * x + y)))
        def _():
            remote(att_all.at[0], att_all.at[head], o_send.at[0, 0], o_recv.at[head], sib).wait_recv()

    for t in range(8):
        two = [att_all[2 * t], att_all[2 * t + 1]]
        for h in range(2):
            rows = [value[:, h * 64 : h * 64 + 64] for value in two]
            lhs[pl.ds(h * HALF, HALF), pl.ds(t * 128, 128)] = jnp.concatenate(rows, axis=1)
    for part_of in range(4):
        value, columns = out_part(128, part_of)
        out_ref[:, columns] = (total[:, columns] + value).astype(BF16)

    acts.finish()
    kv_lats.finish()
    q_lats.finish()
    halo.wait_send()
    for j in range(2):
        @pl.when(jnp.logical_not(jnp.logical_and(even, 2 * c + j == y)))
        def _():
            q_copy(j).wait_send()

        @pl.when(2 * c + j != y)
        def _():
            kv_copy(j).wait_send()

    for qb in range(2):
        for t in range(8):
            @pl.when(jnp.logical_not(is_me(qb, t)))
            def _():
                back(qb, t).wait_send()

    for k in range(1, 8):
        pool_copy(k).wait_send()
    weights_out.finish()
    for b in range(2):
        for way in range(2):
            for s in range(4 if way == b else 3):
                ring_copy(0, way, b, s).wait_send()

    @pl.loop(0, 8)
    def _(zb):
        for b in range(2):
            sib_copy(zb * 4 + 2 * c + b).wait_send()


DMA = pltpu.SemaphoreType.DMA


def params(number):
    return pltpu.CompilerParams(collective_id=number, has_side_effects=True, vmem_limit_bytes=60 * 1024 * 1024)


def local(
    activations, in_gain, w_pool_in, pool_gain, w_qlat, w_kvlat, w_krope, qlat_gain, kvlat_gain,
    w_qup, w_kup, w_vup, qhead_gain, khead_gain, w_out_pool, w_out_attn,
):
    tables = [jnp.asarray(t) for t in rotary_tables()]
    gather_sems = [DMA((6,)), DMA((8,)), DMA((8, 2))]
    return pl.pallas_call(
        mixer_kernel,
        name="mixer",
        out_shape=jax.ShapeDtypeStruct((BLOCK, D), BF16),
        in_specs=[ANY_SPEC if k in (2, 3, 4, 5, 9, 10, 11, 18, 19) else VMEM_SPEC for k in range(20)],
        out_specs=VMEM_SPEC,
        scratch_shapes=[
            pltpu.VMEM((D, 128), BF16),
            pltpu.VMEM((192, D), BF16),
            pltpu.VMEM((192, QLAT), BF16),
            pltpu.VMEM((2, KVLAT, 128), BF16),
            DMA((9,)),
            pltpu.VMEM((8, BLOCK, D), BF16),
            pltpu.VMEM((ROWS, 192), F32),
            pltpu.VMEM((64, ROWS), BF16),
            pltpu.VMEM((8, 64, ROWS), BF16),
            pltpu.VMEM((96, ROWS), BF16),
            pltpu.VMEM((8, 96, ROWS), BF16),
            pltpu.VMEM((HALO + ROWS, 128), F32),
            pltpu.VMEM((HALO, 128), BF16),
            pltpu.VMEM((HALO, 128), BF16),
            pltpu.VMEM((D, 192), BF16),
            pltpu.VMEM((256, KVLAT), BF16),
            pltpu.VMEM((2, HEAD, ROWS), BF16),
            pltpu.VMEM((2, LAT, ROWS), BF16),
            pltpu.VMEM((ROWS, 128), BF16),
            pltpu.VMEM((32, LAT, ROWS), BF16),
            pltpu.VMEM((32, ROWS, HEAD), BF16),
            pltpu.VMEM((2, HEAD, ROWS), BF16),
            pltpu.VMEM((2, VDIM, ROWS), F32),
            pltpu.VMEM((2, 8, ROWS), F32),
            pltpu.VMEM((2, 8, HALF, 128), BF16),
            pltpu.VMEM((16, HALF, 128), BF16),
            pltpu.VMEM((8, BLOCK, 128), BF16),
            pltpu.VMEM((8, 256, D), BF16),
            pltpu.VMEM((BLOCK, D // 2), BF16),
            pltpu.VMEM((BLOCK, D), F32),
            *gather_sems, *gather_sems, *gather_sems, DMA((2,)),
            DMA((2,)), DMA((32,)), DMA((2,)), DMA((2,)), DMA((2, 2, 4)), DMA((32,)), DMA((2, 8)), DMA((16,)),
            DMA((8,)), DMA((8,)), *gather_sems,
        ],
        compiler_params=params(1),
    )(
        activations, in_gain[None, :], w_pool_in, w_qlat.T, w_kvlat.T, w_krope.T, pool_gain[None, :], qlat_gain,
        kvlat_gain[None, :], w_qup.T, w_kup, w_vup, qhead_gain[None, :], khead_gain[None, :], *tables, w_out_pool, w_out_attn,
    )


def solution(mesh):
    placed = (
        P(("sp", "tp"), None), P(), P(None, "tp"), P("tp"), P(None, "tp"), P(None, "tp"), P(), P(), P(),
        P(None, "tp"), P(None, "tp"), P(None, "tp"), P(), P(), P("tp", None), P("tp", None),
    )
    return jax.shard_map(local, mesh=mesh, in_specs=placed, out_specs=P(("sp", "tp"), None), check_vma=False)
```
